512 devices in a mesh: ep: 32 (over z, core), tp: 16 (over y, x).
Axes of the slice: x: 4, y: 4, z: 16, core: 2. Of those that a mesh axis runs over, the one named last changes fastest.
Arguments:
- mixer_input_channels: bfloat16 [8192, 4096], P('ep', 'tp'), may hold values from -6 to 6
- input_state_projection: bfloat16 [8192, 4096], P('ep', 'tp'), may hold values from -6 to 6
- output_state_projection: bfloat16 [8192, 4096], P('ep', 'tp'), may hold values from -6 to 6
- output_gate_logits: bfloat16 [8192, 4096], P('ep', 'tp'), may hold values from -6 to 6
- step_size_logits: float32 [8192, 64], P('ep', 'tp'), may hold values from -4.4 to 2.9
- extra_log_decay: float32 [8192, 64], P('ep', 'tp'), may hold values from -2.1 to 0, as said below
- mixer_channel_taps: bfloat16 [4, 4096], P(None, 'tp'), may hold values from -3 to 3
- input_state_taps: bfloat16 [4, 4096], P(None, 'tp'), may hold values from -3 to 3
- output_state_taps: bfloat16 [4, 4096], P(None, 'tp'), may hold values from -3 to 3
- decay_rate_log: float32 [64], P('tp')
- head_skip_weight: float32 [64], P('tp'), may hold values from 0.1 to 1.9
- grouped_norm_gain: float32 [4096], P('tp'), may hold values from 0.1 to 1.9
- mixer_output_weight: bfloat16 [4096, 2048], P('tp'), may hold values from -0.09375 to 0.09375
- expert_input_tokens: bfloat16 [4096, 2048], P('ep'), may hold values from -6 to 6
- routing: int32 [4096, 2], P('ep'), may hold values from 0 to 31, all different within a row; in each aligned block of 128 rows (0 to 127, 128 to 255, ...) at most 10 rows name the same one
- router_chosen_scores: float32 [4096, 2], P('ep'), may hold values from 0.05 to 1
- expert_norm_gain: float32 [2048], replicated, may hold values from 0.1 to 1.9
- expert_gate_weight: bfloat16 [32, 2048, 2048], P('ep', None, 'tp'), may hold values from -0.125 to 0.125
- expert_up_weight: bfloat16 [32, 2048, 2048], P('ep', None, 'tp'), may hold values from -0.125 to 0.125
- expert_down_weight: bfloat16 [32, 2048, 2048], P('ep', 'tp'), may hold values from -0.125 to 0.125
Outputs:
- mixer_output_first: bfloat16 [8192, 2048], P('ep', 'tp')
- moe_out: bfloat16 [4096, 2048], P('ep', 'tp')
The draws below stay inside these ranges and needn't reach their ends.
Inputs may be any that keep to these rules, and one draw needn't show every extreme that they name: `routing`: within the rows of one index of ep (aligned blocks of 128 rows) no expert is named more than 10 times, some expert exactly 10 times; a row names 2 different experts. `extra_log_decay`: zero at all but a few positions.
All inputs are finite; a program needn't handle non-finite values.
Results may differ from the reference program's by a relative error of at most 0.018.
Values may be sent and summed in bfloat16 or wider, within the bound.
No kernel may reach another device: no remote copies, remote signals or barrier semaphores. Data moves between devices by JAX's collectives and lax.ppermute only.
A program may use at most 64 MiB of HBM per device.

```python
import math
import jax
import jax.numpy as jnp
import numpy as np
from jax import lax

D = 2048
HEADS = 64
HEAD_DIM = 64
GROUPS = 32
STATE = 128
CONV = 4
BLOCK = 128
FF = 2048
TOPK = 2
T_EP = 256
TOK_EP = 128
INNER = 4096
SEQ = 8192
EXPERTS = 32
CAP = 10
MOE_TOKENS = 4096
N_TP = 16


def draw_step_size_logits(key, part):
    spans = SEQ // T_EP
    offsets = jax.random.uniform(jax.random.fold_in(key, 11), (spans, 1), jnp.float32, -2.0, 0.5)
    noise = jnp.clip(0.8 * jax.random.normal(jax.random.fold_in(key, 12), (SEQ, HEADS), jnp.float32), -2.4, 2.4)
    return jnp.repeat(offsets, T_EP, axis=0) + noise


def draw_decay_rate_log(key, part):
    share = 0.5
    fast = jax.random.uniform(jax.random.fold_in(key, 21), (HEADS,), jnp.float32) < share
    quick = jax.random.uniform(jax.random.fold_in(key, 22), (HEADS,), jnp.float32, math.log(1.0 / 100.0), math.log(1.0 / 30.0)) - math.log(0.45)
    slow = jax.random.uniform(jax.random.fold_in(key, 23), (HEADS,), jnp.float32, math.log(0.1), math.log(0.8)) - jnp.log(0.45 * SEQ)
    return jnp.where(fast, quick, slow)


def draw_extra_log_decay(key, part):
    spots = jax.random.randint(jax.random.fold_in(key, 31), (3,), 0, SEQ)
    hit = (jnp.arange(SEQ, dtype=jnp.int32)[:, None] == spots[None, :]).astype(jnp.float32)
    loss = jax.random.uniform(jax.random.fold_in(key, 32), (3, HEADS), jnp.float32, math.log(0.5), math.log(0.8))
    return jnp.dot(hit, loss)


def level_of(key, dims, split, low, largest):
    def one(dim, blocks):
        draws = jax.random.uniform(jax.random.fold_in(jax.random.fold_in(key, 6), dim), (blocks,), jnp.float32, low / len(split), largest / len(split))
        return jnp.repeat(jnp.exp(draws), dims[dim] // blocks).reshape((-1,) + (1,) * (len(dims) - dim - 1))

    loudness = one(*split[0])
    for cut in split[1:]:
        loudness = loudness * one(*cut)
    return loudness


def routed_block(own_key, own, number, rows, number_of, top, limit, skew):
    ranking = jax.random.permutation(own_key, number_of)
    packed, ordinary = load_shares(number_of, rows * top, limit, skew, True), load_shares(number_of, rows * top, limit, skew, False)
    places = jnp.arange(number_of)

    def named(lengths, rotation):
        used = int((lengths > 0).sum())
        fixed = max(1, used // 4)
        shifted = fixed + (places - fixed + rotation * (used - fixed)) % max(1, number_of - fixed)
        return jnp.zeros((number_of,), jnp.int32).at[ranking[jnp.where(places < fixed, places, shifted)]].set(jnp.asarray(lengths, jnp.int32))

    lengths = jnp.where(number % 4 == 0, named(packed, number // 4), named(ordinary, number - number // 4 - 1))
    mixed = jax.random.permutation(jax.random.fold_in(own, 3), number_of)
    giver, taker = mixed[0:number_of // 2 * 2:2], mixed[1:number_of // 2 * 2:2]
    room = jnp.minimum(lengths[giver] - 1, limit - lengths[taker]) // 2
    room = jnp.where((giver == ranking[0]) | (taker == ranking[0]) | (lengths[taker] == 0), 0, jnp.maximum(room, 0))
    shifted = jax.random.randint(jax.random.fold_in(own, 4), (number_of // 2,), 0, 1 << 20) % (room + 1)
    lengths = lengths.at[giver].add(-shifted).at[taker].add(shifted)
    items = jnp.searchsorted(jnp.cumsum(lengths), jnp.arange(rows * top), side="right").astype(jnp.int32)
    table = items.reshape(top, rows).T
    table = table[jax.random.permutation(jax.random.fold_in(own, 1), rows)]
    rotation = jax.random.randint(jax.random.fold_in(own, 2), (rows, 1), 0, top)
    return jnp.take_along_axis(table, (jnp.arange(top)[None, :] + rotation) % top, axis=1)


def load_shares(amount, total, limit, lean, full):
    portions = [(1 << 20) // math.isqrt(grade ** lean) + 1 for grade in range(1, amount + 1)]
    largest = limit if full else min(limit, max(-(-total // amount), total * portions[0] // sum(portions)))
    least = 1 if total - largest >= amount - 1 else 0
    given, surplus = [largest] + [least] * (amount - 1), total - largest - least * (amount - 1)
    while surplus > 0:
        candidates = [i for i in range(1, amount) if given[i] < largest] or [i for i in range(1, amount) if given[i] < limit]
        whole, remaining = sum([portions[i] for i in candidates]), surplus
        for i in candidates:
            addition = min(limit - given[i], max(1, remaining * portions[i] // whole), surplus)
            given[i] = given[i] + addition
            surplus = surplus - addition
    return np.array(given)


def normal_values(key, dims, spread, reach, shards=(), kind=jnp.bfloat16):
    result = spread * jax.random.normal(key, dims, jnp.float32)
    if shards:
        result = result * level_of(key, dims, shards, -0.22, 0.18)
    return jnp.clip(result, -reach, reach).astype(kind)


def setup_inputs(seed: int = 0) -> dict:
    streams_of = jax.random.split(jax.random.key(seed), 21)
    mixer_input_channels = normal_values(streams_of[0], (SEQ, INNER), 1.0, 6.0, ((0, 32), (1, 16)))
    input_state_projection = normal_values(streams_of[1], (SEQ, GROUPS * STATE), 1.0, 6.0, ((0, 32), (1, 16)))
    output_state_projection = normal_values(streams_of[2], (SEQ, GROUPS * STATE), 1.0, 6.0, ((0, 32), (1, 16)))
    output_gate_logits = normal_values(streams_of[3], (SEQ, INNER), 1.0, 6.0, ((0, 32), (1, 16)))
    step_size_logits = draw_step_size_logits(jax.random.fold_in(streams_of[20], 71), 0)
    extra_log_decay = draw_extra_log_decay(jax.random.fold_in(streams_of[20], 71), 0)
    mixer_channel_taps = normal_values(streams_of[6], (CONV, INNER), CONV ** -0.5, 3.0, ((1, 16),))
    input_state_taps = normal_values(streams_of[7], (CONV, GROUPS * STATE), CONV ** -0.5, 3.0, ((1, 16),))
    output_state_taps = normal_values(streams_of[8], (CONV, GROUPS * STATE), CONV ** -0.5, 3.0, ((1, 16),))
    decay_rate_log = draw_decay_rate_log(jax.random.fold_in(streams_of[20], 71), 0)
    head_skip_weight = jnp.clip(1.0 + 0.18 * jax.random.normal(streams_of[10], (HEADS,), jnp.float32), 0.1, 1.9)
    grouped_norm_gain = jnp.clip(1.0 + 0.18 * jax.random.normal(streams_of[11], (INNER,), jnp.float32), 0.1, 1.9)
    mixer_output_weight = normal_values(streams_of[12], (INNER, D), INNER ** -0.5, 0.09375, ((0, 16),))
    expert_input_tokens = normal_values(streams_of[13], (MOE_TOKENS, D), 1.0, 6.0, ((0, 32),))
    routing_keys = jax.random.split(jax.random.fold_in(streams_of[14], 1), MOE_TOKENS // TOK_EP)
    routing_turns = jax.random.permutation(jax.random.fold_in(streams_of[14], 3), MOE_TOKENS // TOK_EP)
    routing = jax.vmap(lambda own, number: routed_block(jax.random.fold_in(streams_of[14], 2), own, number, TOK_EP, EXPERTS, TOPK, CAP, 1))(routing_keys, routing_turns).reshape((MOE_TOKENS, TOPK))
    router_chosen_scores = jnp.clip(jnp.exp(math.log(1.0) - 2.9957323 * jax.random.uniform(streams_of[15], (MOE_TOKENS, TOPK), jnp.float32) ** level_of(streams_of[15], (MOE_TOKENS, TOPK), ((0, 32),), -0.2, 0.2)), 0.05, 1.0)
    expert_norm_gain = jnp.clip(1.0 + 0.18 * jax.random.normal(streams_of[16], (D,), jnp.float32), 0.1, 1.9)
    expert_gate_weight = normal_values(streams_of[17], (EXPERTS, D, FF), D ** -0.5, 0.125, ((0, 32), (2, 16)))
    expert_up_weight = normal_values(streams_of[18], (EXPERTS, D, FF), D ** -0.5, 0.125, ((0, 32), (2, 16)))
    expert_down_weight = normal_values(streams_of[19], (EXPERTS, FF, D), FF ** -0.5, 0.125, ((0, 32), (1, 16)))
    return dict(mixer_input_channels=mixer_input_channels, input_state_projection=input_state_projection, output_state_projection=output_state_projection, output_gate_logits=output_gate_logits, step_size_logits=step_size_logits, extra_log_decay=extra_log_decay, mixer_channel_taps=mixer_channel_taps, input_state_taps=input_state_taps, output_state_taps=output_state_taps, decay_rate_log=decay_rate_log, head_skip_weight=head_skip_weight, grouped_norm_gain=grouped_norm_gain, mixer_output_weight=mixer_output_weight, expert_input_tokens=expert_input_tokens, routing=routing, router_chosen_scores=router_chosen_scores, expert_norm_gain=expert_norm_gain, expert_gate_weight=expert_gate_weight, expert_up_weight=expert_up_weight, expert_down_weight=expert_down_weight)


eps = 1e-06

def causal_conv(values, taps):
    length = values.shape[0]
    padded = jnp.pad(values.astype(jnp.float32), ((taps.shape[0] - 1, 0), (0, 0)))
    total = jnp.zeros(values.shape, jnp.float32)
    for index in range(taps.shape[0]):
        total = total + padded[index:index + length] * taps[index].astype(jnp.float32)
    return jax.nn.silu(total).astype(jnp.bfloat16)

def split_sum(left, right):
    parts_left = jnp.transpose(left.reshape(left.shape[0], N_TP, left.shape[1] // N_TP), (1, 0, 2))
    parts_right = right.reshape(N_TP, right.shape[0] // N_TP, right.shape[1])

    def add_part(total, pair):
        term = jnp.dot(pair[0], pair[1], preferred_element_type=jnp.float32)
        return (total + lax.optimization_barrier(term.astype(jnp.bfloat16)).astype(jnp.float32), None)
    total, _ = lax.scan(add_part, jnp.zeros((left.shape[0], right.shape[1]), jnp.float32), (parts_left, parts_right))
    return total.astype(jnp.bfloat16)

def mixer_baseline(mixer_input_channels, input_state_projection, output_state_projection, output_gate_logits, step_size_logits, extra_log_decay, mixer_channel_taps, input_state_taps, output_state_taps, decay_rate_log, head_skip_weight, grouped_norm_gain, mixer_output_weight):
    length = mixer_input_channels.shape[0]
    blocks = length // BLOCK
    per_group = HEADS // GROUPS
    x_conv = causal_conv(mixer_input_channels, mixer_channel_taps)
    b_conv = causal_conv(input_state_projection, input_state_taps)
    c_conv = causal_conv(output_state_projection, output_state_taps)
    step_size = jax.nn.softplus(step_size_logits)
    head_log_decay = step_size * -jnp.exp(decay_rate_log) + extra_log_decay
    decay_sum = jnp.cumsum(head_log_decay.reshape(blocks, BLOCK, HEADS), axis=1)
    x_blocks = x_conv.reshape(blocks, BLOCK, HEADS, HEAD_DIM)
    x_step = (x_blocks.astype(jnp.float32) * step_size.reshape(blocks, BLOCK, HEADS)[..., None]).astype(jnp.bfloat16)
    b_blocks = b_conv.reshape(blocks, BLOCK, GROUPS, STATE).astype(jnp.float32)
    c_blocks = c_conv.reshape(blocks, BLOCK, GROUPS, STATE).astype(jnp.float32)
    inner = jnp.einsum('blgn,bsgn->bgls', c_blocks, b_blocks)
    across = jnp.transpose(decay_sum, (0, 2, 1)).reshape(blocks, GROUPS, per_group, BLOCK)
    order = jnp.arange(BLOCK, dtype=jnp.int32)
    causal = order[:, None] >= order[None, :]
    distance = across[..., :, None] - across[..., None, :]
    decay = jnp.where(causal, jnp.exp(jnp.where(causal, distance, 0.0)), 0.0)
    scores = (inner[:, :, None] * decay).astype(jnp.bfloat16).reshape(blocks, HEADS, BLOCK, BLOCK)
    y_diag = jnp.einsum('bhls,bshp->blhp', scores.astype(jnp.float32), x_step.astype(jnp.float32))
    block_last = decay_sum[:, -1]
    x_weighted = (x_step.astype(jnp.float32) * jnp.exp(block_last[:, None, :] - decay_sum)[..., None]).astype(jnp.bfloat16)
    states = jnp.einsum('blgn,blgep->bgepn', b_blocks, x_weighted.reshape(blocks, BLOCK, GROUPS, per_group, HEAD_DIM).astype(jnp.float32))
    states = states.reshape(blocks, HEADS, HEAD_DIM, STATE)

    def carry_step(state, inputs):
        return (state * jnp.exp(inputs[1])[:, None, None] + inputs[0], state)
    _, entering = lax.scan(carry_step, jnp.zeros((HEADS, HEAD_DIM, STATE), jnp.float32), (states, block_last))
    entering = entering.astype(jnp.bfloat16)
    y_off = jnp.einsum('blgn,bgepn->blgep', c_blocks, entering.reshape(blocks, GROUPS, per_group, HEAD_DIM, STATE).astype(jnp.float32))
    y_off = y_off.reshape(blocks, BLOCK, HEADS, HEAD_DIM) * jnp.exp(decay_sum)[..., None]
    mixed = (y_diag + y_off + head_skip_weight[:, None] * x_blocks.astype(jnp.float32)).reshape(length, HEADS * HEAD_DIM)
    mixed = mixed * jax.nn.silu(output_gate_logits.astype(jnp.float32))
    grouped = mixed.reshape(length, GROUPS, per_group * HEAD_DIM)
    grouped = grouped * lax.rsqrt(lax.optimization_barrier(jnp.mean(grouped * grouped, axis=-1, keepdims=True)) + eps)
    mix_normed = (grouped.reshape(length, HEADS * HEAD_DIM) * grouped_norm_gain).astype(jnp.bfloat16)
    return split_sum(mix_normed, mixer_output_weight)

def expert_reference(expert_input_tokens, routing, router_chosen_scores, expert_norm_gain, expert_gate_weight, expert_up_weight, expert_down_weight):
    count = expert_input_tokens.shape[0]
    sources = count // TOK_EP
    rows = expert_input_tokens.astype(jnp.float32)
    normed = (rows * lax.rsqrt(lax.optimization_barrier(jnp.mean(rows * rows, axis=-1, keepdims=True)) + eps) * expert_norm_gain).astype(jnp.bfloat16)
    flat = routing.reshape(sources, TOK_EP * TOPK)
    member = (flat[..., None] == jnp.arange(EXPERTS, dtype=jnp.int32)).astype(jnp.int32)
    rank = lax.optimization_barrier(jnp.sum((jnp.cumsum(member, axis=1) - member) * member, axis=2))
    slot = (jnp.arange(sources, dtype=jnp.int32)[:, None] * CAP + rank).reshape(count, TOPK).astype(jnp.int32)
    owner = jnp.broadcast_to(jnp.arange(count, dtype=jnp.int32)[:, None], (count, TOPK))
    table = jnp.zeros((EXPERTS, sources * CAP), jnp.int32).at[routing, slot].set(owner)

    def one_expert(inputs):
        index, gate_w, up_w, down_w = inputs
        chosen = normed[index]
        gate = jnp.dot(chosen, gate_w, preferred_element_type=jnp.float32)
        up = jnp.dot(chosen, up_w, preferred_element_type=jnp.float32)
        hidden = (jax.nn.silu(gate) * up).astype(jnp.bfloat16)
        return split_sum(hidden, down_w)
    results = lax.map(one_expert, (table, expert_gate_weight, expert_up_weight, expert_down_weight))
    picked = results[routing, slot].astype(jnp.float32)
    share = router_chosen_scores / lax.optimization_barrier(jnp.sum(router_chosen_scores, axis=1, keepdims=True))
    return lax.optimization_barrier(jnp.sum(share[..., None] * picked, axis=1)).astype(jnp.bfloat16)

def reference(mixer_input_channels, input_state_projection, output_state_projection, output_gate_logits, step_size_logits, extra_log_decay, mixer_channel_taps, input_state_taps, output_state_taps, decay_rate_log, head_skip_weight, grouped_norm_gain, mixer_output_weight, expert_input_tokens, routing, router_chosen_scores, expert_norm_gain, expert_gate_weight, expert_up_weight, expert_down_weight):
    mixer_output_first = mixer_baseline(mixer_input_channels, input_state_projection, output_state_projection, output_gate_logits, step_size_logits, extra_log_decay, mixer_channel_taps, input_state_taps, output_state_taps, decay_rate_log, head_skip_weight, grouped_norm_gain, mixer_output_weight)
    moe_out = expert_reference(expert_input_tokens, routing, router_chosen_scores, expert_norm_gain, expert_gate_weight, expert_up_weight, expert_down_weight)
    return (mixer_output_first, moe_out)
```

```python
import functools

import jax
import jax.numpy as jnp
from jax import lax
from jax.experimental import pallas as pl
from jax.experimental.pallas import tpu as pltpu
from jax.sharding import Mesh
from jax.sharding import PartitionSpec as P

HEAD_DIM = 64
STATE = 128
BLOCK = 128
EP = ("ep_0", "ep_1")
SLOTS = 16
LOG_ROW = 10
VMEM = 16 << 20
F32 = jnp.float32
BF16 = jnp.bfloat16

eps = 1e-06


def iota(shape, dim):
    return lax.broadcasted_iota(jnp.int32, shape, dim)


def dot(a, b, ca=1, cb=0, precision=None):
    return lax.dot_general(
        a, b, (((ca,), (cb,)), ((), ())), precision=precision, preferred_element_type=F32
    )


def silu(x):
    return x * (1.0 / (1.0 + jnp.exp(-x)))


def softplus(x):
    return jnp.maximum(x, 0.0) + jnp.log1p(jnp.exp(-jnp.abs(x)))


def kernel_call(body, outs, args, flops, scratch=()):
    size = sum(a.size * a.dtype.itemsize for a in args)
    size += sum(o.size * o.dtype.itemsize for o in outs)
    return pl.pallas_call(
        body,
        out_shape=outs,
        in_specs=[pl.BlockSpec(memory_space=pltpu.VMEM)] * len(args),
        out_specs=[pl.BlockSpec(memory_space=pltpu.VMEM)] * len(outs),
        scratch_shapes=scratch,
        cost_estimate=pl.CostEstimate(flops=flops, bytes_accessed=size, transcendentals=0),
        compiler_params=pltpu.CompilerParams(vmem_limit_bytes=VMEM),
    )(*args)


def shape(dims, kind):
    return jax.ShapeDtypeStruct(dims, kind)


def slots_of(routing_ref):
    tokens = routing_ref.shape[0]
    expert = iota((tokens, 128), 1)
    first = expert == routing_ref[:, 0:1]
    second = expert == routing_ref[:, 1:2]
    member = jnp.where(first | second, 1.0, 0.0).astype(BF16)
    earlier = jnp.where(iota((tokens, tokens), 0) > iota((tokens, tokens), 1), 1.0, 0.0)
    place = dot(earlier.astype(BF16), member) + (expert * SLOTS).astype(F32)
    return [
        jnp.sum(jnp.where(chosen, place, 0.0), axis=1, keepdims=True).astype(jnp.int32)
        for chosen in (first, second)
    ]


def log_decay_of(step_ref, extra_ref, rate_ref):
    step = softplus(step_ref[...])
    return step, step * -jnp.exp(rate_ref[...]) + extra_ref[...]


def dispatch_body(tok_ref, gain_ref, routing_ref, step_ref, extra_ref, rate_ref, out_ref, wide):
    tokens, model = tok_ref.shape
    rows = tok_ref[...].astype(F32)
    scale = lax.rsqrt(jnp.sum(rows * rows, axis=1, keepdims=True) * (1.0 / model) + eps)
    columns = pl.ds(pl.multiple_of(lax.axis_index("tp") * 128, 128), 128)
    own = (tok_ref[:, columns].astype(F32) * scale * gain_ref[:, columns]).astype(BF16)
    slots = slots_of(routing_ref)
    total = out_ref.shape[0]
    place = iota((tokens, total), 1)
    pick = jnp.where((place == slots[0]) | (place == slots[1]), 1.0, 0.0).astype(BF16)
    sent = dot(pick, own, 0, 0)
    _, log_decay = log_decay_of(step_ref, extra_ref, rate_ref)
    heads = log_decay.shape[1]
    left = jnp.sum(log_decay, axis=0, keepdims=True)
    wide[...] = jnp.zeros_like(wide)
    for part in range(3):
        piece = left.astype(BF16).astype(F32)
        wide[part : part + 1, 0:heads] = piece
        left = left - piece
    sent = sent.reshape(total // SLOTS, SLOTS, 128)
    row = iota(sent.shape, 1)
    for part in range(3):
        sent = jnp.where(row == LOG_ROW + part, wide[part : part + 1, :][None], sent)
    out_ref[...] = sent.reshape(total, 128).astype(BF16)


def spread_body(capacity, in_ref, out_ref):
    count = out_ref.shape[1]
    row = iota((count, in_ref.shape[0]), 0)
    source = row // capacity * SLOTS + row % capacity
    pick = jnp.where(iota(source.shape, 1) == source, 1.0, 0.0).astype(BF16)
    packed = dot(pick, in_ref[...]).astype(BF16)
    for peer in range(out_ref.shape[0]):
        out_ref[peer] = packed


def ffn_body(in_ref, gate_ref, up_ref, down_ref, out_ref):
    parts, rows, width = in_ref.shape
    total = jnp.zeros((rows, 2 * width), F32)
    for k in range(0, parts, 2):
        left = jnp.concatenate([in_ref[k], in_ref[k + 1]], axis=1)
        span = pl.ds(k * width, 2 * width)
        right = jnp.concatenate([gate_ref[span, :], up_ref[span, :]], axis=1)
        total = total + dot(left, right)
    hidden = (silu(total[:, :width]) * total[:, width:]).astype(BF16)
    for k in range(0, parts, 2):
        value = dot(hidden, down_ref[:, k * width : (k + 2) * width]).astype(BF16)
        out_ref[k] = value[:, :width]
        out_ref[k + 1] = value[:, width:]


def sum_of(in_ref):
    total = in_ref[0].astype(F32)
    for k in range(1, in_ref.shape[0]):
        total = total + in_ref[k].astype(F32)
    return total.astype(BF16)


def expert_sum_body(capacity, in_ref, out_ref):
    total = sum_of(in_ref)
    count = total.shape[0]
    row = iota((out_ref.shape[0], count), 0)
    source = jnp.where(row % SLOTS < capacity, row // SLOTS * capacity + row % SLOTS, -1)
    pick = jnp.where(iota(source.shape, 1) == source, 1.0, 0.0).astype(BF16)
    out_ref[...] = dot(pick, total).astype(BF16)


def sum_body(in_ref, out_ref):
    out_ref[...] = sum_of(in_ref)


def combine_body(table_ref, routing_ref, score_ref, out_ref):
    tokens = routing_ref.shape[0]
    scores = score_ref[...]
    whole = scores[:, 0:1] + scores[:, 1:2]
    place = iota((tokens, table_ref.shape[0]), 1)
    total = jnp.zeros(out_ref.shape, F32)
    for index, slot in enumerate(slots_of(routing_ref)):
        pick = jnp.where(place == slot, 1.0, 0.0).astype(BF16)
        total = total + scores[:, index : index + 1] / whole * dot(pick, table_ref[...])
    out_ref[...] = total.astype(BF16)


def conv_silu(values_ref, prior_ref, taps_ref, start, held):
    length = values_ref.shape[0]
    reach = taps_ref.shape[0] - 1
    held[8 - reach : 8, :] = prior_ref[start : start + reach, :].astype(F32)
    held[8 : 8 + length, :] = values_ref[...].astype(F32)
    total = jnp.zeros(values_ref.shape, F32)
    for k in range(reach + 1):
        total = total + held[8 - reach + k : 8 - reach + k + length, :] * taps_ref[
            k : k + 1, :
        ].astype(F32)
    return silu(total).astype(BF16)


def running_sum(values):
    length = values.shape[0]
    reach = 1
    row = iota(values.shape, 0)
    while reach < length:
        moved = pltpu.roll(values, reach, 0)
        values = values + jnp.where(row >= reach, moved, 0.0)
        reach *= 2
    return values


def pair(left, right, dims, dim):
    return jnp.where(iota(dims, dim) < HEAD_DIM, left, right)


def block_terms(block, step_all, log_all):
    rows = slice(block * BLOCK, (block + 1) * BLOCK)
    step = step_all[rows]
    decay = running_sum(log_all[rows])
    return rows, step, decay, decay[BLOCK - 1 : BLOCK, :]


def states_body(
    x_ref, b_ref, c_ref, prior_ref, xt_ref, bt_ref, ct_ref, step_ref, extra_ref, rate_ref,
    xo_ref, bo_ref, co_ref, first_ref, total_ref, held,
):
    xo_ref[...] = conv_silu(x_ref, prior_ref, xt_ref, 0, held)
    bo_ref[...] = conv_silu(b_ref, prior_ref, bt_ref, 3, held)
    co_ref[...] = conv_silu(c_ref, prior_ref, ct_ref, 6, held)
    step_all, log_all = log_decay_of(step_ref, extra_ref, rate_ref)
    wide = (BLOCK, 128)
    for group in range(x_ref.shape[1] // 128):
        columns = slice(group * 128, (group + 1) * 128)
        a, b = 2 * group, 2 * group + 1
        state = None
        for block in range(x_ref.shape[0] // BLOCK):
            rows, step, decay, last = block_terms(block, step_all, log_all)
            x = xo_ref[rows, columns].astype(F32)
            x_step = (x * pair(step[:, a : a + 1], step[:, b : b + 1], wide, 1)).astype(BF16)
            left = jnp.exp(last - decay)
            weighted = x_step.astype(F32) * pair(left[:, a : a + 1], left[:, b : b + 1], wide, 1)
            new = dot(weighted.astype(BF16), bo_ref[rows, columns], 0, 0)
            if state is None:
                first_ref[columns, :] = new
                state = new
            else:
                kept = jnp.exp(last)
                state = state * pair(kept[:, a : a + 1], kept[:, b : b + 1], wide, 0) + new
        total_ref[columns, :] = state.astype(BF16)


def carry_body(moved_ref, table_ref, out_ref):
    sources = table_ref.shape[0] // SLOTS
    rows = moved_ref.shape[0] // sources
    me = lax.axis_index("ep_0") * 2 + lax.axis_index("ep_1")
    head = me * rows // HEAD_DIM
    sent = table_ref[...].reshape(sources, SLOTS, 128).astype(F32)
    row, lane = iota(sent.shape, 1), iota(sent.shape, 2)
    wanted = (row >= LOG_ROW) & (row < LOG_ROW + 3) & (lane == head)
    logs = jnp.sum(jnp.sum(jnp.where(wanted, sent, 0.0), axis=2, keepdims=True), axis=1)
    decay = jnp.exp(logs)
    state = jnp.zeros((rows, 128), F32)
    for k in range(sources):
        place = slice(k * rows, (k + 1) * rows)
        out_ref[place, :] = state.astype(BF16)
        state = state * decay[k : k + 1, :] + moved_ref[place, :].astype(F32)


def mixer_body(
    x_ref, b_ref, c_ref, gate_ref, first_ref, income_ref, step_ref, extra_ref, rate_ref,
    skip_ref, gain_ref, weight_ref, out_ref, normed,
):
    step_all, log_all = log_decay_of(step_ref, extra_ref, rate_ref)
    wide = (BLOCK, 128)
    causal = iota(wide, 0) >= iota(wide, 1)
    for block in range(x_ref.shape[0] // BLOCK):
        rows, step, decay, last = block_terms(block, step_all, log_all)
        grown = jnp.exp(decay)
        for group in range(x_ref.shape[1] // 128):
            columns = slice(group * 128, (group + 1) * 128)
            a, b = 2 * group, 2 * group + 1
            x = x_ref[rows, columns].astype(F32)
            x_step = (x * pair(step[:, a : a + 1], step[:, b : b + 1], wide, 1)).astype(BF16)
            c = c_ref[rows, columns]
            inner = dot(c, b_ref[rows, columns], 1, 1)
            parts = []
            for head in (a, b):
                along = jnp.broadcast_to(decay[:, head : head + 1], wide)
                distance = along - along.T
                scale = jnp.where(causal, jnp.exp(jnp.where(causal, distance, 0.0)), 0.0)
                parts.append(dot((inner * scale).astype(BF16), x_step))
            y = pair(parts[0], parts[1], wide, 1)
            entering = income_ref[columns, :].astype(F32)
            if block > 0:
                entering = entering * pair(kept[:, a : a + 1], kept[:, b : b + 1], wide, 0)
                entering = entering + first_ref[columns, :]
            off = dot(c, entering.astype(BF16), 1, 1)
            off = off * pair(grown[:, a : a + 1], grown[:, b : b + 1], wide, 1)
            skip = pair(skip_ref[:, a : a + 1], skip_ref[:, b : b + 1], wide, 1)
            mixed = (y + off + skip * x) * silu(gate_ref[rows, columns].astype(F32))
            mean = jnp.sum(mixed * mixed, axis=1, keepdims=True) * (1.0 / 128)
            mixed = mixed * lax.rsqrt(mean + eps) * gain_ref[:, columns]
            normed[rows, columns] = mixed.astype(BF16)
        kept = jnp.exp(last)
    for k in range(0, out_ref.shape[0], 2):
        value = dot(normed[...], weight_ref[:, k * 128 : (k + 2) * 128]).astype(BF16)
        out_ref[k] = value[:, :128]
        out_ref[k + 1] = value[:, 128:]


def all_to_all(value, axis):
    return lax.all_to_all(value, axis, split_axis=0, concat_axis=0, tiled=True)


def per_device(
    mixer_input_channels,
    input_state_projection,
    output_state_projection,
    output_gate_logits,
    step_size_logits,
    extra_log_decay,
    mixer_channel_taps,
    input_state_taps,
    output_state_taps,
    decay_rate_log,
    head_skip_weight,
    grouped_norm_gain,
    mixer_output_weight,
    expert_input_tokens,
    routing,
    router_chosen_scores,
    expert_norm_gain,
    expert_gate_weight,
    expert_up_weight,
    expert_down_weight,
):
    parts = lax.axis_size("tp")
    devices = lax.axis_size(EP)
    length, channels = mixer_input_channels.shape
    reach = mixer_channel_taps.shape[0] - 1
    tokens, model = expert_input_tokens.shape
    top = routing.shape[1]
    capacity = (tokens * top * 5 + 4 * devices - 1) // (4 * devices)
    slots = devices * SLOTS
    rate, skip = decay_rate_log[None], head_skip_weight[None]

    edge = jnp.concatenate(
        [
            v[length - reach :]
            for v in (mixer_input_channels, input_state_projection, output_state_projection)
        ],
        axis=0,
    )
    prior = lax.ppermute(edge, EP, [(i, i + 1) for i in range(devices - 1)])

    (outgoing,) = kernel_call(
        dispatch_body,
        [shape((slots, 128), BF16)],
        (expert_input_tokens, expert_norm_gain[None], routing, step_size_logits, extra_log_decay, rate),
        2 * slots * tokens * 128,
        [pltpu.VMEM((8, 128), F32)],
    )
    arrived = all_to_all(outgoing.reshape(devices, SLOTS, 128), EP).reshape(slots, 128)

    x_conv, b_conv, c_conv, first, total = kernel_call(
        states_body,
        [shape((length, channels), BF16)] * 3
        + [shape((channels, STATE), F32), shape((channels, STATE), BF16)],
        (
            mixer_input_channels, input_state_projection, output_state_projection, prior,
            mixer_channel_taps, input_state_taps, output_state_taps,
            step_size_logits, extra_log_decay, rate,
        ),
        2 * length * channels * STATE,
        [pltpu.VMEM((length + 8, channels), F32)],
    )
    piece = channels // devices
    moved = all_to_all(total.reshape(devices, piece, STATE), EP).reshape(channels, STATE)

    (copies,) = kernel_call(
        functools.partial(spread_body, capacity),
        [shape((parts, devices * capacity, 128), BF16)],
        (arrived,),
        2 * slots * devices * capacity * 128,
    )
    gathered = all_to_all(copies, "tp")

    (carried,) = kernel_call(
        carry_body, [shape((channels, STATE), BF16)], (moved, arrived), 4 * channels * STATE
    )
    income = all_to_all(carried.reshape(devices, piece, STATE), EP).reshape(channels, STATE)

    (partial_rows,) = kernel_call(
        ffn_body,
        [shape((parts, devices * capacity, 128), BF16)],
        (gathered, expert_gate_weight[0], expert_up_weight[0], expert_down_weight[0]),
        6 * devices * capacity * model * 128,
    )
    expert_parts = all_to_all(partial_rows, "tp")

    (mixer_part,) = kernel_call(
        mixer_body,
        [shape((parts, length, 128), BF16)],
        (
            x_conv, b_conv, c_conv, output_gate_logits, first, income,
            step_size_logits, extra_log_decay, rate, skip, grouped_norm_gain[None],
            mixer_output_weight,
        ),
        2 * length * channels * model,
        [pltpu.VMEM((length, channels), BF16)],
    )
    mixer_parts = all_to_all(mixer_part, "tp")

    (back,) = kernel_call(
        functools.partial(expert_sum_body, capacity),
        [shape((slots, 128), BF16)],
        (expert_parts,),
        2 * slots * devices * capacity * 128,
    )
    table = all_to_all(back.reshape(devices, SLOTS, 128), EP).reshape(slots, 128)

    (mixer_output_first,) = kernel_call(
        sum_body, [shape((length, 128), BF16)], (mixer_parts,), parts * length * 128
    )
    (moe_out,) = kernel_call(
        combine_body,
        [shape((tokens, 128), BF16)],
        (table, routing, router_chosen_scores),
        4 * tokens * slots * 128,
    )
    return (mixer_output_first, moe_out)


def solution(mesh):
    split = Mesh(mesh.devices.reshape(16, 2, mesh.shape["tp"]), ("ep_0", "ep_1", "tp"))
    in_specs = (
        P(EP, "tp"),
        P(EP, "tp"),
        P(EP, "tp"),
        P(EP, "tp"),
        P(EP, "tp"),
        P(EP, "tp"),
        P(None, "tp"),
        P(None, "tp"),
        P(None, "tp"),
        P("tp"),
        P("tp"),
        P("tp"),
        P("tp", None),
        P(EP, None),
        P(EP, None),
        P(EP, None),
        P(),
        P(EP, None, "tp"),
        P(EP, None, "tp"),
        P(EP, "tp", None),
    )
    out_specs = (P(EP, "tp"), P(EP, "tp"))
    return jax.shard_map(
        per_device, mesh=split, in_specs=in_specs, out_specs=out_specs, check_vma=False
    )
```

```python
import functools

import jax
import jax.numpy as jnp
from jax import lax
from jax.experimental import pallas as pl
from jax.experimental.pallas import tpu as pltpu
from jax.sharding import Mesh
from jax.sharding import PartitionSpec as P

HEAD_DIM = 64
STATE = 128
BLOCK = 128
CHIPS = "ep_0"
EP = (CHIPS, "core")
SLOTS = 16
NOTE = 16
VMEM = 16 << 20
WHOLE_VMEM = 60 << 20
F32 = jnp.float32
BF16 = jnp.bfloat16

eps = 1e-06


def iota(shape, dim):
    return lax.broadcasted_iota(jnp.int32, shape, dim)


def dot(a, b, ca=1, cb=0, precision=None):
    return lax.dot_general(
        a, b, (((ca,), (cb,)), ((), ())), precision=precision, preferred_element_type=F32
    )


def silu(x):
    return x * (1.0 / (1.0 + jnp.exp(-x)))


def softplus(x):
    return jnp.maximum(x, 0.0) + jnp.log1p(jnp.exp(-jnp.abs(x)))


def fetched(body, ins, outs, own, far, late):
    def whole(*refs):
        given, rest = list(refs[:ins]), refs[ins : ins + outs + own]
        held, sems = refs[ins + outs + own : -1], refs[-1]
        copies = {}
        for k, index in enumerate(far):
            source = given[index]
            if source.shape != held[k].shape:
                source = source.at[pl.ds(source.shape[0] - held[k].shape[0], held[k].shape[0]), :]
            copies[index] = pltpu.make_async_copy(source, held[k], sems.at[k])
            copies[index].start()
            given[index] = held[k]
        for index in far:
            if index not in late:
                copies[index].wait()
        body(*given, *rest, *(copies[index].wait for index in late))

    return whole


def kernel_call(body, outs, args, flops, scratch=(), far=(), late=(), tails=(), vmem=VMEM):
    size = sum(a.size * a.dtype.itemsize for a in args)
    size += sum(o.size * o.dtype.itemsize for o in outs)
    specs = [
        pl.BlockSpec(memory_space=pltpu.HBM if k in far else pltpu.VMEM) for k in range(len(args))
    ]
    scratch = list(scratch)
    if far:
        body = fetched(body, len(args), len(outs), len(scratch), far, late)
        for k in far:
            dims = (8, args[k].shape[1]) if k in tails else args[k].shape
            scratch.append(pltpu.VMEM(dims, args[k].dtype))
        scratch.append(pltpu.SemaphoreType.DMA((len(far),)))
    return pl.pallas_call(
        body,
        out_shape=outs,
        in_specs=specs,
        out_specs=[pl.BlockSpec(memory_space=pltpu.VMEM)] * len(outs),
        scratch_shapes=scratch,
        cost_estimate=pl.CostEstimate(flops=flops, bytes_accessed=size, transcendentals=0),
        compiler_params=pltpu.CompilerParams(vmem_limit_bytes=vmem),
    )(*args)


def shape(dims, kind):
    return jax.ShapeDtypeStruct(dims, kind)


def upright(ref):
    wide = jnp.concatenate([ref[...].astype(F32)] * (8 // ref.shape[0]), axis=0)
    return wide.T[:, : ref.shape[0]]


def slots_of(routing_ref):
    tokens = routing_ref.shape[1]
    expert = iota((tokens, 128), 1)
    named = upright(routing_ref).astype(jnp.int32)
    first = expert == named[:, 0:1]
    second = expert == named[:, 1:2]
    member = jnp.where(first | second, 1.0, 0.0).astype(BF16)
    earlier = jnp.where(iota((tokens, tokens), 0) > iota((tokens, tokens), 1), 1.0, 0.0)
    place = dot(earlier.astype(BF16), member) + (expert * SLOTS).astype(F32)
    return [
        jnp.sum(jnp.where(chosen, place, 0.0), axis=1, keepdims=True).astype(jnp.int32)
        for chosen in (first, second)
    ]


def log_decay_of(step_ref, extra_ref, rate_ref):
    step = softplus(upright(step_ref))
    return step, step * -jnp.exp(rate_ref[...]) + upright(extra_ref)


def dispatch_body(
    tok_ref, gain_ref, routing_ref, x_ref, b_ref, c_ref, out_ref, edge_ref
):
    tokens, model = tok_ref.shape
    rows = tok_ref[...].astype(F32)
    scale = lax.rsqrt(jnp.sum(rows * rows, axis=1, keepdims=True) * (1.0 / model) + eps)
    columns = pl.ds(pl.multiple_of(lax.axis_index("tp") * 128, 128), 128)
    own = (tok_ref[:, columns].astype(F32) * scale * gain_ref[:, columns]).astype(BF16)
    slots = slots_of(routing_ref)
    place = iota((tokens, out_ref.shape[0]), 1)
    pick = jnp.where((place == slots[0]) | (place == slots[1]), 1.0, 0.0).astype(BF16)
    out_ref[...] = dot(pick, own, 0, 0).astype(BF16)
    for k, ref in enumerate((x_ref, b_ref, c_ref)):
        edge_ref[8 * k : 8 * k + 8, :] = ref[...]


def spread_body(capacity, in_ref, out_ref):
    count = out_ref.shape[1]
    row = iota((count, in_ref.shape[0]), 0)
    source = row // capacity * SLOTS + row % capacity
    pick = jnp.where(iota(source.shape, 1) == source, 1.0, 0.0).astype(BF16)
    packed = dot(pick, in_ref[...]).astype(BF16)
    for peer in range(out_ref.shape[0]):
        out_ref[peer] = packed


def ffn_body(in_ref, gate_ref, up_ref, down_ref, out_ref, wait):
    parts, rows, width = in_ref.shape
    total = jnp.zeros((rows, 2 * width), F32)
    for k in range(0, parts, 2):
        left = jnp.concatenate([in_ref[k], in_ref[k + 1]], axis=1)
        span = pl.ds(k * width, 2 * width)
        right = jnp.concatenate([gate_ref[span, :], up_ref[span, :]], axis=1)
        total = total + dot(left, right)
    hidden = (silu(total[:, :width]) * total[:, width:]).astype(BF16)
    wait()
    for k in range(0, parts, 2):
        value = dot(hidden, down_ref[:, k * width : (k + 2) * width]).astype(BF16)
        out_ref[k] = value[:, :width]
        out_ref[k + 1] = value[:, width:]


def sum_of(in_ref):
    total = in_ref[0].astype(F32)
    for k in range(1, in_ref.shape[0]):
        total = total + in_ref[k].astype(F32)
    return total.astype(BF16)


def expert_sum_body(capacity, in_ref, out_ref):
    total = sum_of(in_ref)
    count = total.shape[0]
    row = iota((out_ref.shape[0], count), 0)
    source = jnp.where(row % SLOTS < capacity, row // SLOTS * capacity + row % SLOTS, -1)
    pick = jnp.where(iota(source.shape, 1) == source, 1.0, 0.0).astype(BF16)
    out_ref[...] = dot(pick, total).astype(BF16)


def sum_body(in_ref, out_ref):
    out_ref[...] = sum_of(in_ref)


def combine_body(table_ref, routing_ref, score_ref, out_ref):
    tokens = routing_ref.shape[1]
    scores = upright(score_ref)
    whole = scores[:, 0:1] + scores[:, 1:2]
    place = iota((tokens, table_ref.shape[0]), 1)
    total = jnp.zeros(out_ref.shape, F32)
    for index, slot in enumerate(slots_of(routing_ref)):
        pick = jnp.where(place == slot, 1.0, 0.0).astype(BF16)
        total = total + scores[:, index : index + 1] / whole * dot(pick, table_ref[...])
    out_ref[...] = total.astype(BF16)


def conv_silu(values_ref, prior_ref, taps_ref, start, held):
    length = values_ref.shape[0]
    reach = taps_ref.shape[0] - 1
    held[0:8, :] = prior_ref[start : start + 8, :].astype(F32)
    held[8 : 8 + length, :] = values_ref[...].astype(F32)
    total = jnp.zeros(values_ref.shape, F32)
    for k in range(reach + 1):
        total = total + held[8 - reach + k : 8 - reach + k + length, :] * taps_ref[
            k : k + 1, :
        ].astype(F32)
    return silu(total).astype(BF16)


def running_sum(values):
    length = values.shape[0]
    reach = 1
    row = iota(values.shape, 0)
    while reach < length:
        moved = pltpu.roll(values, reach, 0)
        values = values + jnp.where(row >= reach, moved, 0.0)
        reach *= 2
    return values


def pair(left, right, dims, dim):
    return jnp.where(iota(dims, dim) < HEAD_DIM, left, right)


def block_terms(block, step_all, log_all):
    rows = slice(block * BLOCK, (block + 1) * BLOCK)
    step = step_all[rows]
    decay = running_sum(log_all[rows])
    return rows, step, decay, decay[BLOCK - 1 : BLOCK, :]


def states_body(
    x_ref, b_ref, c_ref, prior_ref, xt_ref, bt_ref, ct_ref, step_ref, extra_ref, rate_ref,
    xo_ref, bo_ref, co_ref, first_ref, total_ref, held, wide_ref,
):
    xo_ref[...] = conv_silu(x_ref, prior_ref, xt_ref, 0, held)
    bo_ref[...] = conv_silu(b_ref, prior_ref, bt_ref, 8, held)
    co_ref[...] = conv_silu(c_ref, prior_ref, ct_ref, 16, held)
    step_all, log_all = log_decay_of(step_ref, extra_ref, rate_ref)
    wide = (BLOCK, 128)
    for group in range(x_ref.shape[1] // 128):
        columns = slice(group * 128, (group + 1) * 128)
        a, b = 2 * group, 2 * group + 1
        state = None
        for block in range(x_ref.shape[0] // BLOCK):
            rows, step, decay, last = block_terms(block, step_all, log_all)
            x = xo_ref[rows, columns].astype(F32)
            x_step = (x * pair(step[:, a : a + 1], step[:, b : b + 1], wide, 1)).astype(BF16)
            left = jnp.exp(last - decay)
            weighted = x_step.astype(F32) * pair(left[:, a : a + 1], left[:, b : b + 1], wide, 1)
            new = dot(weighted.astype(BF16), bo_ref[rows, columns], 0, 0)
            if state is None:
                first_ref[columns, :] = new
                state = new
            else:
                kept = jnp.exp(last)
                state = state * pair(kept[:, a : a + 1], kept[:, b : b + 1], wide, 0) + new
        total_ref[columns, :] = state.astype(BF16)
    write_log(total_ref, jnp.sum(log_all, axis=0, keepdims=True), wide_ref)


def write_log(ref, log, wide_ref):
    rows = ref.shape[0] - NOTE
    wide_ref[...] = jnp.zeros_like(wide_ref)
    for part in range(3):
        piece = log.astype(ref.dtype).astype(F32)
        wide_ref[part : part + 1, 0 : log.shape[1]] = piece
        log = log - piece
    ref[rows:, :] = wide_ref[...].astype(ref.dtype)


def by_row(values, rows):
    head = iota((rows, 128), 0) // HEAD_DIM
    total = jnp.broadcast_to(values[:, 0:1], (rows, 128))
    for k in range(1, values.shape[1]):
        total = jnp.where(head == k, values[:, k : k + 1], total)
    return total


def read(part):
    rows = part.shape[0] - NOTE
    note = part[rows:, :].astype(F32)
    log = (note[0:1] + note[1:2] + note[2:3])[:, : rows // HEAD_DIM]
    return part[:rows, :].astype(F32), log


def joined(earlier, later):
    decay = by_row(jnp.exp(later[1]), later[0].shape[0])
    return earlier[0] * decay + later[0], earlier[1] + later[1]


def write(ref, value, wide_ref):
    ref[: ref.shape[0] - NOTE, :] = value[0].astype(ref.dtype)
    write_log(ref, value[1], wide_ref)


def join_core_body(both_ref, out_ref, wide_ref):
    write(out_ref, joined(read(both_ref[0]), read(both_ref[1])), wide_ref)


def join_first_body(came_ref, own_ref, out_ref, wide_ref):
    write(out_ref, joined(read(came_ref[...]), read(own_ref[...])), wide_ref)


def join_body(came_ref, own_ref, before_ref, out_ref, new_ref, wide_ref):
    came = read(came_ref[...])
    write(out_ref, joined(came, read(own_ref[...])), wide_ref)
    write(new_ref, joined(came, read(before_ref[...])), wide_ref)


def income_of(came_ref, before_ref, both_ref):
    state = joined(read(came_ref[...]), read(before_ref[...]))
    inside = joined(state, read(both_ref[0]))
    return jnp.where(lax.axis_index("core") == 1, inside[0], state[0])


def mixer_body(
    x_ref, b_ref, c_ref, gate_ref, first_ref, came_ref, before_ref, both_ref, step_ref, extra_ref,
    rate_ref, skip_ref, gain_ref, weight_ref, out_ref, normed, income_ref,
):
    income_ref[...] = income_of(came_ref, before_ref, both_ref)
    step_all, log_all = log_decay_of(step_ref, extra_ref, rate_ref)
    wide = (BLOCK, 128)
    causal = iota(wide, 0) >= iota(wide, 1)
    for block in range(x_ref.shape[0] // BLOCK):
        rows, step, decay, last = block_terms(block, step_all, log_all)
        grown = jnp.exp(decay)
        for group in range(x_ref.shape[1] // 128):
            columns = slice(group * 128, (group + 1) * 128)
            a, b = 2 * group, 2 * group + 1
            x = x_ref[rows, columns].astype(F32)
            x_step = (x * pair(step[:, a : a + 1], step[:, b : b + 1], wide, 1)).astype(BF16)
            c = c_ref[rows, columns]
            inner = dot(c, b_ref[rows, columns], 1, 1)
            parts = []
            for head in (a, b):
                along = jnp.broadcast_to(decay[:, head : head + 1], wide)
                distance = along - along.T
                scale = jnp.where(causal, jnp.exp(jnp.where(causal, distance, 0.0)), 0.0)
                parts.append(dot((inner * scale).astype(BF16), x_step))
            y = pair(parts[0], parts[1], wide, 1)
            entering = income_ref[columns, :]
            if block > 0:
                entering = entering * pair(kept[:, a : a + 1], kept[:, b : b + 1], wide, 0)
                entering = entering + first_ref[columns, :]
            off = dot(c, entering.astype(BF16), 1, 1)
            off = off * pair(grown[:, a : a + 1], grown[:, b : b + 1], wide, 1)
            skip = pair(skip_ref[:, a : a + 1], skip_ref[:, b : b + 1], wide, 1)
            mixed = (y + off + skip * x) * silu(gate_ref[rows, columns].astype(F32))
            mean = jnp.sum(mixed * mixed, axis=1, keepdims=True) * (1.0 / 128)
            mixed = mixed * lax.rsqrt(mean + eps) * gain_ref[:, columns]
            normed[rows, columns] = mixed.astype(BF16)
        kept = jnp.exp(last)
    for k in range(0, out_ref.shape[0], 2):
        value = dot(normed[...], weight_ref[:, k * 128 : (k + 2) * 128]).astype(BF16)
        out_ref[k] = value[:, :128]
        out_ref[k + 1] = value[:, 128:]


def all_to_all(value, axis):
    return lax.all_to_all(value, axis, split_axis=0, concat_axis=0, tiled=True)


def per_device(
    mixer_input_channels,
    input_state_projection,
    output_state_projection,
    output_gate_logits,
    step_size_logits,
    extra_log_decay,
    mixer_channel_taps,
    input_state_taps,
    output_state_taps,
    decay_rate_log,
    head_skip_weight,
    grouped_norm_gain,
    mixer_output_weight,
    expert_input_tokens,
    routing,
    router_chosen_scores,
    expert_norm_gain,
    expert_gate_weight,
    expert_up_weight,
    expert_down_weight,
):
    parts = lax.axis_size("tp")
    devices = lax.axis_size(EP)
    length, channels = mixer_input_channels.shape
    tokens, model = expert_input_tokens.shape
    top = routing.shape[1]
    capacity = (tokens * top * 5 + 4 * devices - 1) // (4 * devices)
    slots = devices * SLOTS
    rate, skip = decay_rate_log[None], head_skip_weight[None]
    step_rows, extra_rows = step_size_logits.T, extra_log_decay.T
    routing_rows = routing.T

    outgoing, edge = kernel_call(
        dispatch_body,
        [shape((slots, 128), BF16), shape((24, channels), BF16)],
        (
            expert_input_tokens, expert_norm_gain[None], routing_rows,
            mixer_input_channels, input_state_projection, output_state_projection,
        ),
        2 * slots * tokens * 128,
        far=(0, 1, 2, 3, 4, 5),
        tails=(3, 4, 5),
        vmem=WHOLE_VMEM,
    )
    prior = lax.ppermute(edge, EP, [(i, i + 1) for i in range(devices - 1)])
    arrived = all_to_all(outgoing.reshape(devices, SLOTS, 128), EP)
    arrived = arrived.reshape(slots, 128)

    note = channels + NOTE
    wide = pltpu.VMEM((NOTE, 128), F32)
    x_conv, b_conv, c_conv, first, total = kernel_call(
        states_body,
        [shape((length, channels), BF16)] * 3
        + [shape((channels, STATE), F32), shape((note, STATE), BF16)],
        (
            mixer_input_channels, input_state_projection, output_state_projection, prior,
            mixer_channel_taps, input_state_taps, output_state_taps,
            step_rows, extra_rows, rate,
        ),
        2 * length * channels * STATE,
        [pltpu.VMEM((length + 8, channels), F32), wide],
        far=(0, 1, 2, 4, 5, 6, 7, 8, 9),
        vmem=WHOLE_VMEM,
    )

    def moved(value, distance):
        chips = lax.axis_size(CHIPS)
        route = [(i, i + distance) for i in range(chips - distance)]
        return lax.ppermute(value, CHIPS, route)

    def join(body, values, more=()):
        outs = [shape((note, STATE), BF16), *more]
        return kernel_call(body, outs, values, 4 * channels * STATE, [wide])

    both = lax.all_gather(total, "core")
    (upto,) = join(join_core_body, (both,))
    before = came = moved(upto, 1)
    (upto,) = join(join_first_body, (came, upto))
    for distance in (2, 4):
        came = moved(upto, distance)
        upto, before = join(join_body, (came, upto, before), [shape((note, STATE), F32)])
    came = moved(upto, 8)

    (copies,) = kernel_call(
        functools.partial(spread_body, capacity),
        [shape((parts, devices * capacity, 128), BF16)],
        (arrived,),
        2 * slots * devices * capacity * 128,
    )
    gathered = all_to_all(copies, "tp")

    (partial_rows,) = kernel_call(
        ffn_body,
        [shape((parts, devices * capacity, 128), BF16)],
        (gathered, expert_gate_weight[0], expert_up_weight[0], expert_down_weight[0]),
        6 * devices * capacity * model * 128,
        far=(3,),
        late=(3,),
    )
    expert_parts = all_to_all(partial_rows, "tp")

    (mixer_part,) = kernel_call(
        mixer_body,
        [shape((parts, length, 128), BF16)],
        (
            x_conv, b_conv, c_conv, output_gate_logits, first, came, before, both,
            step_rows, extra_rows, rate, skip, grouped_norm_gain[None], mixer_output_weight,
        ),
        2 * length * channels * model,
        [pltpu.VMEM((length, channels), BF16), pltpu.VMEM((channels, STATE), F32)],
    )
    mixer_parts = all_to_all(mixer_part, "tp")

    (back,) = kernel_call(
        functools.partial(expert_sum_body, capacity),
        [shape((slots, 128), BF16)],
        (expert_parts,),
        2 * slots * devices * capacity * 128,
    )
    table = all_to_all(back.reshape(devices, SLOTS, 128), EP).reshape(slots, 128)

    (mixer_output_first,) = kernel_call(
        sum_body, [shape((length, 128), BF16)], (mixer_parts,), parts * length * 128
    )
    (moe_out,) = kernel_call(
        combine_body,
        [shape((tokens, 128), BF16)],
        (table, routing_rows, router_chosen_scores.T),
        4 * tokens * slots * 128,
    )
    return (mixer_output_first, moe_out)


def solution(mesh):
    split = Mesh(mesh.devices.reshape(16, 2, mesh.shape["tp"]), (*EP, "tp"))
    in_specs = (
        P(EP, "tp"),
        P(EP, "tp"),
        P(EP, "tp"),
        P(EP, "tp"),
        P(EP, "tp"),
        P(EP, "tp"),
        P(None, "tp"),
        P(None, "tp"),
        P(None, "tp"),
        P("tp"),
        P("tp"),
        P("tp"),
        P("tp", None),
        P(EP, None),
        P(EP, None),
        P(EP, None),
        P(),
        P(EP, None, "tp"),
        P(EP, None, "tp"),
        P(EP, "tp", None),
    )
    out_specs = (P(EP, "tp"), P(EP, "tp"))
    return jax.shard_map(
        per_device, mesh=split, in_specs=in_specs, out_specs=out_specs, check_vma=False
    )
```

```python
import functools

import jax
import jax.numpy as jnp
from jax import lax
from jax.experimental import pallas as pl
from jax.experimental.pallas import tpu as pltpu
from jax.sharding import Mesh
from jax.sharding import PartitionSpec as P

HEAD_DIM = 64
STATE = 128
BLOCK = 128
CHIPS = "ep_0"
EP = (CHIPS, "core")
SLOTS = 16
SIDE = 4
NOTE = 16
VMEM = 16 << 20
WHOLE_VMEM = 60 << 20
F32 = jnp.float32
BF16 = jnp.bfloat16

eps = 1e-06


def iota(shape, dim):
    return lax.broadcasted_iota(jnp.int32, shape, dim)


def dot(a, b, ca=1, cb=0, precision=None):
    return lax.dot_general(
        a, b, (((ca,), (cb,)), ((), ())), precision=precision, preferred_element_type=F32
    )


def silu(x):
    return x * (1.0 / (1.0 + jnp.exp(-x)))


def softplus(x):
    return jnp.maximum(x, 0.0) + jnp.log1p(jnp.exp(-jnp.abs(x)))


def fetched(body, ins, outs, own, far, late):
    def whole(*refs):
        given, rest = list(refs[:ins]), refs[ins : ins + outs + own]
        held, sems = refs[ins + outs + own : -1], refs[-1]
        copies = {}
        for k, index in enumerate(far):
            source = given[index]
            if source.shape != held[k].shape:
                source = source.at[pl.ds(source.shape[0] - held[k].shape[0], held[k].shape[0]), :]
            copies[index] = pltpu.make_async_copy(source, held[k], sems.at[k])
            copies[index].start()
            given[index] = held[k]
        for index in far:
            if index not in late:
                copies[index].wait()
        body(*given, *rest, *(copies[index].wait for index in late))

    return whole


def kernel_call(body, outs, args, flops, scratch=(), far=(), late=(), tails=(), vmem=VMEM):
    size = sum(a.size * a.dtype.itemsize for a in args)
    size += sum(o.size * o.dtype.itemsize for o in outs)
    specs = [
        pl.BlockSpec(memory_space=pltpu.HBM if k in far else pltpu.VMEM) for k in range(len(args))
    ]
    scratch = list(scratch)
    if far:
        body = fetched(body, len(args), len(outs), len(scratch), far, late)
        for k in far:
            dims = (8, args[k].shape[1]) if k in tails else args[k].shape
            scratch.append(pltpu.VMEM(dims, args[k].dtype))
        scratch.append(pltpu.SemaphoreType.DMA((len(far),)))
    return pl.pallas_call(
        body,
        out_shape=outs,
        in_specs=specs,
        out_specs=[pl.BlockSpec(memory_space=pltpu.VMEM)] * len(outs),
        scratch_shapes=scratch,
        cost_estimate=pl.CostEstimate(flops=flops, bytes_accessed=size, transcendentals=0),
        compiler_params=pltpu.CompilerParams(vmem_limit_bytes=vmem),
    )(*args)


def shape(dims, kind):
    return jax.ShapeDtypeStruct(dims, kind)


def upright(ref):
    wide = jnp.concatenate([ref[...].astype(F32)] * (8 // ref.shape[0]), axis=0)
    return wide.T[:, : ref.shape[0]]


def slots_of(routing_ref):
    tokens = routing_ref.shape[1]
    expert = iota((tokens, 128), 1)
    named = upright(routing_ref).astype(jnp.int32)
    first = expert == named[:, 0:1]
    second = expert == named[:, 1:2]
    member = jnp.where(first | second, 1.0, 0.0).astype(BF16)
    earlier = jnp.where(iota((tokens, tokens), 0) > iota((tokens, tokens), 1), 1.0, 0.0)
    place = dot(earlier.astype(BF16), member) + (expert * SLOTS).astype(F32)
    return [
        jnp.sum(jnp.where(chosen, place, 0.0), axis=1, keepdims=True).astype(jnp.int32)
        for chosen in (first, second)
    ]


def log_decay_of(step_ref, extra_ref, rate_ref):
    step = softplus(upright(step_ref))
    return step, step * -jnp.exp(rate_ref[...]) + upright(extra_ref)


def dispatch_body(
    tok_ref, gain_ref, routing_ref, x_ref, b_ref, c_ref, out_ref, edge_ref
):
    tokens, model = tok_ref.shape
    rows = tok_ref[...].astype(F32)
    scale = lax.rsqrt(jnp.sum(rows * rows, axis=1, keepdims=True) * (1.0 / model) + eps)
    columns = pl.ds(pl.multiple_of(lax.axis_index("tp") * 128, 128), 128)
    own = (tok_ref[:, columns].astype(F32) * scale * gain_ref[:, columns]).astype(BF16)
    slots = slots_of(routing_ref)
    place = iota((tokens, out_ref.shape[0]), 1)
    pick = jnp.where((place == slots[0]) | (place == slots[1]), 1.0, 0.0).astype(BF16)
    out_ref[...] = dot(pick, own, 0, 0).astype(BF16)
    for k, ref in enumerate((x_ref, b_ref, c_ref)):
        edge_ref[8 * k : 8 * k + 8, :] = ref[...]


def spread_body(capacity, in_ref, out_ref):
    count = out_ref.shape[1]
    row = iota((count, in_ref.shape[0]), 0)
    source = row // capacity * SLOTS + row % capacity
    pick = jnp.where(iota(source.shape, 1) == source, 1.0, 0.0).astype(BF16)
    packed = dot(pick, in_ref[...]).astype(BF16)
    for peer in range(out_ref.shape[0]):
        out_ref[peer] = packed


def ffn_body(in_ref, gate_ref, up_ref, down_ref, out_ref, wait):
    parts, rows, width = in_ref.shape
    total = jnp.zeros((rows, 2 * width), F32)
    for k in range(0, parts, 2):
        left = jnp.concatenate([in_ref[k], in_ref[k + 1]], axis=1)
        span = pl.ds(k * width, 2 * width)
        right = jnp.concatenate([gate_ref[span, :], up_ref[span, :]], axis=1)
        total = total + dot(left, right)
    hidden = (silu(total[:, :width]) * total[:, width:]).astype(BF16)
    wait()
    for k in range(0, parts, 2):
        value = dot(hidden, down_ref[:, k * width : (k + 2) * width]).astype(BF16)
        out_ref[k] = value[:, :width]
        out_ref[k + 1] = value[:, width:]


def sum_of(in_ref):
    total = in_ref[0].astype(F32)
    for k in range(1, in_ref.shape[0]):
        total = total + in_ref[k].astype(F32)
    return total.astype(BF16)


def expert_sum_body(capacity, in_ref, out_ref):
    total = sum_of(in_ref)
    count = total.shape[0]
    row = iota((out_ref.shape[0], count), 0)
    source = jnp.where(row % SLOTS < capacity, row // SLOTS * capacity + row % SLOTS, -1)
    pick = jnp.where(iota(source.shape, 1) == source, 1.0, 0.0).astype(BF16)
    out_ref[...] = dot(pick, total).astype(BF16)


def combine_body(table_ref, routing_ref, score_ref, out_ref):
    tokens = routing_ref.shape[1]
    scores = upright(score_ref)
    whole = scores[:, 0:1] + scores[:, 1:2]
    place = iota((tokens, table_ref.shape[0]), 1)
    total = jnp.zeros(out_ref.shape, F32)
    for index, slot in enumerate(slots_of(routing_ref)):
        pick = jnp.where(place == slot, 1.0, 0.0).astype(BF16)
        total = total + scores[:, index : index + 1] / whole * dot(pick, table_ref[...])
    out_ref[...] = total.astype(BF16)


def conv_silu(values_ref, prior_ref, taps_ref, start, held):
    length = values_ref.shape[0]
    reach = taps_ref.shape[0] - 1
    held[0:8, :] = prior_ref[start : start + 8, :].astype(F32)
    held[8 : 8 + length, :] = values_ref[...].astype(F32)
    total = jnp.zeros(values_ref.shape, F32)
    for k in range(reach + 1):
        total = total + held[8 - reach + k : 8 - reach + k + length, :] * taps_ref[
            k : k + 1, :
        ].astype(F32)
    return silu(total).astype(BF16)


def running_sum(values):
    length = values.shape[0]
    reach = 1
    row = iota(values.shape, 0)
    while reach < length:
        moved = pltpu.roll(values, reach, 0)
        values = values + jnp.where(row >= reach, moved, 0.0)
        reach *= 2
    return values


def pair(left, right, dims, dim):
    return jnp.where(iota(dims, dim) < HEAD_DIM, left, right)


def block_terms(block, step_all, log_all):
    rows = slice(block * BLOCK, (block + 1) * BLOCK)
    step = step_all[rows]
    decay = running_sum(log_all[rows])
    return rows, step, decay, decay[BLOCK - 1 : BLOCK, :]


def states_body(
    x_ref, b_ref, c_ref, prior_ref, xt_ref, bt_ref, ct_ref, step_ref, extra_ref, rate_ref,
    xo_ref, bo_ref, co_ref, first_ref, total_ref, held, wide_ref,
):
    xo_ref[...] = conv_silu(x_ref, prior_ref, xt_ref, 0, held)
    bo_ref[...] = conv_silu(b_ref, prior_ref, bt_ref, 8, held)
    co_ref[...] = conv_silu(c_ref, prior_ref, ct_ref, 16, held)
    step_all, log_all = log_decay_of(step_ref, extra_ref, rate_ref)
    wide = (BLOCK, 128)
    for group in range(x_ref.shape[1] // 128):
        columns = slice(group * 128, (group + 1) * 128)
        a, b = 2 * group, 2 * group + 1
        state = None
        for block in range(x_ref.shape[0] // BLOCK):
            rows, step, decay, last = block_terms(block, step_all, log_all)
            x = xo_ref[rows, columns].astype(F32)
            x_step = (x * pair(step[:, a : a + 1], step[:, b : b + 1], wide, 1)).astype(BF16)
            left = jnp.exp(last - decay)
            weighted = x_step.astype(F32) * pair(left[:, a : a + 1], left[:, b : b + 1], wide, 1)
            new = dot(weighted.astype(BF16), bo_ref[rows, columns], 0, 0)
            if state is None:
                first_ref[columns, :] = new
                state = new
            else:
                kept = jnp.exp(last)
                state = state * pair(kept[:, a : a + 1], kept[:, b : b + 1], wide, 0) + new
        total_ref[columns, :] = state.astype(BF16)
    write_log(total_ref, jnp.sum(log_all, axis=0, keepdims=True), wide_ref)


def write_log(ref, log, wide_ref):
    rows = ref.shape[0] - NOTE
    wide_ref[...] = jnp.zeros_like(wide_ref)
    for part in range(3):
        piece = log.astype(ref.dtype).astype(F32)
        wide_ref[part : part + 1, 0 : log.shape[1]] = piece
        log = log - piece
    ref[rows:, :] = wide_ref[...].astype(ref.dtype)


def by_row(values, rows):
    head = iota((rows, 128), 0) // HEAD_DIM
    total = jnp.broadcast_to(values[:, 0:1], (rows, 128))
    for k in range(1, values.shape[1]):
        total = jnp.where(head == k, values[:, k : k + 1], total)
    return total


def read(part):
    rows = part.shape[0] - NOTE
    note = part[rows:, :].astype(F32)
    log = (note[0:1] + note[1:2] + note[2:3])[:, : rows // HEAD_DIM]
    return part[:rows, :].astype(F32), log


def joined(earlier, later):
    decay = by_row(jnp.exp(later[1]), later[0].shape[0])
    return earlier[0] * decay + later[0], earlier[1] + later[1]


def write(ref, value, wide_ref):
    ref[: ref.shape[0] - NOTE, :] = value[0].astype(ref.dtype)
    write_log(ref, value[1], wide_ref)


def join_core_body(both_ref, out_ref, wide_ref):
    write(out_ref, joined(read(both_ref[0]), read(both_ref[1])), wide_ref)


def join_first_body(came_ref, own_ref, out_ref, wide_ref):
    write(out_ref, joined(read(came_ref[...]), read(own_ref[...])), wide_ref)


def join_body(came_ref, own_ref, before_ref, out_ref, new_ref, wide_ref):
    came = read(came_ref[...])
    write(out_ref, joined(came, read(own_ref[...])), wide_ref)
    write(new_ref, joined(came, read(before_ref[...])), wide_ref)


def income_of(came_ref, before_ref, both_ref):
    state = joined(read(came_ref[...]), read(before_ref[...]))
    inside = joined(state, read(both_ref[0]))
    return jnp.where(lax.axis_index("core") == 1, inside[0], state[0])


def mixer_body(
    x_ref, b_ref, c_ref, gate_ref, first_ref, came_ref, before_ref, both_ref, step_ref, extra_ref,
    rate_ref, skip_ref, gain_ref, weight_ref, *rest,
):
    outs, (normed, income_ref) = rest[:SIDE], rest[SIDE:]
    income_ref[...] = income_of(came_ref, before_ref, both_ref)
    step_all, log_all = log_decay_of(step_ref, extra_ref, rate_ref)
    wide = (BLOCK, 128)
    causal = iota(wide, 0) >= iota(wide, 1)
    for block in range(x_ref.shape[0] // BLOCK):
        rows, step, decay, last = block_terms(block, step_all, log_all)
        grown = jnp.exp(decay)
        for group in range(x_ref.shape[1] // 128):
            columns = slice(group * 128, (group + 1) * 128)
            a, b = 2 * group, 2 * group + 1
            x = x_ref[rows, columns].astype(F32)
            x_step = (x * pair(step[:, a : a + 1], step[:, b : b + 1], wide, 1)).astype(BF16)
            c = c_ref[rows, columns]
            inner = dot(c, b_ref[rows, columns], 1, 1)
            parts = []
            for head in (a, b):
                along = jnp.broadcast_to(decay[:, head : head + 1], wide)
                distance = along - along.T
                scale = jnp.where(causal, jnp.exp(jnp.where(causal, distance, 0.0)), 0.0)
                parts.append(dot((inner * scale).astype(BF16), x_step))
            y = pair(parts[0], parts[1], wide, 1)
            entering = income_ref[columns, :]
            if block > 0:
                entering = entering * pair(kept[:, a : a + 1], kept[:, b : b + 1], wide, 0)
                entering = entering + first_ref[columns, :]
            off = dot(c, entering.astype(BF16), 1, 1)
            off = off * pair(grown[:, a : a + 1], grown[:, b : b + 1], wide, 1)
            skip = pair(skip_ref[:, a : a + 1], skip_ref[:, b : b + 1], wide, 1)
            mixed = (y + off + skip * x) * silu(gate_ref[rows, columns].astype(F32))
            mean = jnp.sum(mixed * mixed, axis=1, keepdims=True) * (1.0 / 128)
            mixed = mixed * lax.rsqrt(mean + eps) * gain_ref[:, columns]
            normed[rows, columns] = mixed.astype(BF16)
        kept = jnp.exp(last)
    y, x = lax.axis_index("tp") // SIDE, lax.axis_index("tp") % SIDE

    def columns_of(up, across):
        part = (y + up) % SIDE * SIDE + (x + across) % SIDE
        return weight_ref[:, pl.ds(pl.multiple_of(part * 128, 128), 128)]

    for across, out_ref in enumerate(outs):
        for up in range(0, SIDE, 2):
            both = jnp.concatenate([columns_of(up, across), columns_of(up + 1, across)], axis=1)
            value = dot(normed[...], both).astype(BF16)
            out_ref[up] = value[:, :128]
            out_ref[up + 1] = value[:, 128:]


def across_body(*refs):
    for up in range(SIDE):
        total = refs[0][up].astype(F32)
        for k in range(1, SIDE):
            total = total + refs[k][up].astype(F32)
        refs[SIDE + up][...] = total.astype(BF16)


def upward_body(*refs):
    total = refs[0][...].astype(F32)
    for k in range(1, SIDE):
        total = total + refs[k][...].astype(F32)
    refs[SIDE][...] = total.astype(BF16)


def all_to_all(value, axis):
    return lax.all_to_all(value, axis, split_axis=0, concat_axis=0, tiled=True)


def per_device(
    mixer_input_channels,
    input_state_projection,
    output_state_projection,
    output_gate_logits,
    step_size_logits,
    extra_log_decay,
    mixer_channel_taps,
    input_state_taps,
    output_state_taps,
    decay_rate_log,
    head_skip_weight,
    grouped_norm_gain,
    mixer_output_weight,
    expert_input_tokens,
    routing,
    router_chosen_scores,
    expert_norm_gain,
    expert_gate_weight,
    expert_up_weight,
    expert_down_weight,
):
    parts = lax.axis_size("tp")
    devices = lax.axis_size(EP)
    length, channels = mixer_input_channels.shape
    tokens, model = expert_input_tokens.shape
    top = routing.shape[1]
    capacity = (tokens * top * 5 + 4 * devices - 1) // (4 * devices)
    slots = devices * SLOTS
    rate, skip = decay_rate_log[None], head_skip_weight[None]
    step_rows, extra_rows = step_size_logits.T, extra_log_decay.T
    routing_rows = routing.T

    outgoing, edge = kernel_call(
        dispatch_body,
        [shape((slots, 128), BF16), shape((24, channels), BF16)],
        (
            expert_input_tokens, expert_norm_gain[None], routing_rows,
            mixer_input_channels, input_state_projection, output_state_projection,
        ),
        2 * slots * tokens * 128,
        far=(0, 1, 2, 3, 4, 5),
        tails=(3, 4, 5),
        vmem=WHOLE_VMEM,
    )
    prior = lax.ppermute(edge, EP, [(i, i + 1) for i in range(devices - 1)])
    arrived = all_to_all(outgoing.reshape(devices, SLOTS, 128), EP)
    arrived = arrived.reshape(slots, 128)

    note = channels + NOTE
    wide = pltpu.VMEM((NOTE, 128), F32)
    x_conv, b_conv, c_conv, first, total = kernel_call(
        states_body,
        [shape((length, channels), BF16)] * 3
        + [shape((channels, STATE), F32), shape((note, STATE), BF16)],
        (
            mixer_input_channels, input_state_projection, output_state_projection, prior,
            mixer_channel_taps, input_state_taps, output_state_taps,
            step_rows, extra_rows, rate,
        ),
        2 * length * channels * STATE,
        [pltpu.VMEM((length + 8, channels), F32), wide],
        far=(0, 1, 2, 4, 5, 6, 7, 8, 9),
        vmem=WHOLE_VMEM,
    )

    def moved(value, distance):
        chips = lax.axis_size(CHIPS)
        route = [(i, i + distance) for i in range(chips - distance)]
        return lax.ppermute(value, CHIPS, route)

    def join(body, values, more=()):
        outs = [shape((note, STATE), BF16), *more]
        return kernel_call(body, outs, values, 4 * channels * STATE, [wide])

    both = lax.all_gather(total, "core")
    (upto,) = join(join_core_body, (both,))
    before = came = moved(upto, 1)
    (upto,) = join(join_first_body, (came, upto))
    for distance in (2, 4):
        came = moved(upto, distance)
        upto, before = join(join_body, (came, upto, before), [shape((note, STATE), F32)])
    came = moved(upto, 8)

    (copies,) = kernel_call(
        functools.partial(spread_body, capacity),
        [shape((parts, devices * capacity, 128), BF16)],
        (arrived,),
        2 * slots * devices * capacity * 128,
    )
    gathered = all_to_all(copies, "tp")

    (partial_rows,) = kernel_call(
        ffn_body,
        [shape((parts, devices * capacity, 128), BF16)],
        (gathered, expert_gate_weight[0], expert_up_weight[0], expert_down_weight[0]),
        6 * devices * capacity * model * 128,
        far=(3,),
        late=(3,),
    )
    expert_parts = all_to_all(partial_rows, "tp")

    mixer_parts = kernel_call(
        mixer_body,
        [shape((SIDE, length, 128), BF16)] * SIDE,
        (
            x_conv, b_conv, c_conv, output_gate_logits, first, came, before, both,
            step_rows, extra_rows, rate, skip, grouped_norm_gain[None], mixer_output_weight,
        ),
        2 * length * channels * model,
        [pltpu.VMEM((length, channels), BF16), pltpu.VMEM((channels, STATE), F32)],
    )

    (back,) = kernel_call(
        functools.partial(expert_sum_body, capacity),
        [shape((slots, 128), BF16)],
        (expert_parts,),
        2 * slots * devices * capacity * 128,
    )
    table = all_to_all(back.reshape(devices, SLOTS, 128), EP).reshape(slots, 128)

    def passed(value, up, across):
        route = [
            (y * SIDE + x, (y + up) % SIDE * SIDE + (x + across) % SIDE)
            for y in range(SIDE)
            for x in range(SIDE)
        ]
        return lax.ppermute(value, "tp", route)

    came = [passed(mixer_parts[k], 0, k) for k in range(1, SIDE)]
    mixer_parts = kernel_call(
        across_body,
        [shape((length, 128), BF16)] * SIDE,
        (mixer_parts[0], *came),
        parts * length * 128,
    )
    came = [passed(mixer_parts[k], k, 0) for k in range(1, SIDE)]
    (mixer_output_first,) = kernel_call(
        upward_body, [shape((length, 128), BF16)], (mixer_parts[0], *came), SIDE * length * 128
    )
    (moe_out,) = kernel_call(
        combine_body,
        [shape((tokens, 128), BF16)],
        (table, routing_rows, router_chosen_scores.T),
        4 * tokens * slots * 128,
    )
    return (mixer_output_first, moe_out)


def solution(mesh):
    split = Mesh(mesh.devices.reshape(16, 2, mesh.shape["tp"]), (*EP, "tp"))
    in_specs = (
        P(EP, "tp"),
        P(EP, "tp"),
        P(EP, "tp"),
        P(EP, "tp"),
        P(EP, "tp"),
        P(EP, "tp"),
        P(None, "tp"),
        P(None, "tp"),
        P(None, "tp"),
        P("tp"),
        P("tp"),
        P("tp"),
        P("tp", None),
        P(EP, None),
        P(EP, None),
        P(EP, None),
        P(),
        P(EP, None, "tp"),
        P(EP, None, "tp"),
        P(EP, "tp", None),
    )
    out_specs = (P(EP, "tp"), P(EP, "tp"))
    return jax.shard_map(
        per_device, mesh=split, in_specs=in_specs, out_specs=out_specs, check_vma=False
    )
```

```python
import jax
import jax.numpy as jnp
from jax import lax
from jax.experimental import pallas as pl
from jax.experimental.pallas import tpu as pltpu
from jax.sharding import Mesh
from jax.sharding import PartitionSpec as P

HEAD_DIM = 64
STATE = 128
BLOCK = 128
CHIPS = "ep_0"
EP = (CHIPS, "core")
LANES = 128
PACK = 2
NOTE = 16
VMEM = 16 << 20
WHOLE_VMEM = 60 << 20
F32 = jnp.float32
BF16 = jnp.bfloat16

eps = 1e-06


def iota(shape, dim):
    return lax.broadcasted_iota(jnp.int32, shape, dim)


def dot(a, b, ca=1, cb=0, precision=None):
    return lax.dot_general(
        a, b, (((ca,), (cb,)), ((), ())), precision=precision, preferred_element_type=F32
    )


def silu(x):
    return x * (1.0 / (1.0 + jnp.exp(-x)))


def softplus(x):
    return jnp.maximum(x, 0.0) + jnp.log1p(jnp.exp(-jnp.abs(x)))


def fetched(body, ins, outs, own, far, late):
    def whole(*refs):
        given, rest = list(refs[:ins]), refs[ins : ins + outs + own]
        held, sems = refs[ins + outs + own : -1], refs[-1]
        copies = {}
        for k, index in enumerate(far):
            source = given[index]
            if source.shape != held[k].shape:
                source = source.at[pl.ds(source.shape[0] - held[k].shape[0], held[k].shape[0]), :]
            copies[index] = pltpu.make_async_copy(source, held[k], sems.at[k])
            copies[index].start()
            given[index] = held[k]
        for index in far:
            if index not in late:
                copies[index].wait()
        body(*given, *rest, *(copies[index].wait for index in late))

    return whole


def kernel_call(body, outs, args, flops, scratch=(), far=(), late=(), tails=(), vmem=VMEM):
    size = sum(a.size * a.dtype.itemsize for a in args)
    size += sum(o.size * o.dtype.itemsize for o in outs)
    specs = [
        pl.BlockSpec(memory_space=pltpu.HBM if k in far else pltpu.VMEM) for k in range(len(args))
    ]
    scratch = list(scratch)
    if far:
        body = fetched(body, len(args), len(outs), len(scratch), far, late)
        for k in far:
            dims = (8, args[k].shape[1]) if k in tails else args[k].shape
            scratch.append(pltpu.VMEM(dims, args[k].dtype))
        scratch.append(pltpu.SemaphoreType.DMA((len(far),)))
    return pl.pallas_call(
        body,
        out_shape=outs,
        in_specs=specs,
        out_specs=[pl.BlockSpec(memory_space=pltpu.VMEM)] * len(outs),
        scratch_shapes=scratch,
        cost_estimate=pl.CostEstimate(flops=flops, bytes_accessed=size, transcendentals=0),
        compiler_params=pltpu.CompilerParams(vmem_limit_bytes=vmem),
    )(*args)


def shape(dims, kind):
    return jax.ShapeDtypeStruct(dims, kind)


def upright(ref):
    wide = jnp.concatenate([ref[...].astype(F32)] * (8 // ref.shape[0]), axis=0)
    return wide.T[:, : ref.shape[0]]


def slots_of(routing_ref, experts):
    tokens = routing_ref.shape[1]
    expert = iota((tokens, 128), 1)
    named = upright(routing_ref).astype(jnp.int32)
    first = expert == named[:, 0:1]
    second = expert == named[:, 1:2]
    member = jnp.where(first | second, 1.0, 0.0).astype(BF16)
    earlier = jnp.where(iota((tokens, tokens), 0) > iota((tokens, tokens), 1), 1.0, 0.0)
    place = dot(earlier.astype(BF16), member)
    slots = []
    for index, chosen in enumerate((first, second)):
        rank = jnp.sum(jnp.where(chosen, place, 0.0), axis=1, keepdims=True).astype(jnp.int32)
        number = named[:, index : index + 1] * PACK + rank % PACK
        slots.append(rank // PACK * (PACK * experts) + number)
    return slots


def pack_rows(rows, held, out_ref):
    experts = out_ref.shape[0]
    span = PACK * experts
    for k in range(out_ref.shape[2] // LANES):
        held[:, k * LANES : (k + 1) * LANES] = rows[k * span : (k + 1) * span, :]
    for e in range(experts):
        out_ref[e] = held[PACK * e : PACK * (e + 1), :]


def unpack_rows(in_ref, held):
    for e in range(in_ref.shape[0]):
        held[PACK * e : PACK * (e + 1), :] = in_ref[e]
    parts = [held[:, k : k + LANES] for k in range(0, in_ref.shape[2], LANES)]
    return jnp.concatenate(parts, axis=0)


def log_decay_of(step_ref, extra_ref, rate_ref):
    step = softplus(upright(step_ref))
    return step, step * -jnp.exp(rate_ref[...]) + upright(extra_ref)


def dispatch_body(
    tok_ref, gain_ref, routing_ref, x_ref, b_ref, c_ref, out_ref, edge_ref, held
):
    tokens, model = tok_ref.shape
    rows = tok_ref[...].astype(F32)
    scale = lax.rsqrt(jnp.sum(rows * rows, axis=1, keepdims=True) * (1.0 / model) + eps)
    columns = pl.ds(pl.multiple_of(lax.axis_index("tp") * 128, 128), 128)
    own = (tok_ref[:, columns].astype(F32) * scale * gain_ref[:, columns]).astype(BF16)
    experts = out_ref.shape[0]
    slots = slots_of(routing_ref, experts)
    place = iota((tokens, out_ref.shape[1] * experts * out_ref.shape[2] // LANES), 1)
    pick = jnp.where((place == slots[0]) | (place == slots[1]), 1.0, 0.0).astype(BF16)
    pack_rows(dot(pick, own, 0, 0).astype(BF16), held, out_ref)
    for k, ref in enumerate((x_ref, b_ref, c_ref)):
        edge_ref[8 * k : 8 * k + 8, :] = ref[...]


def spread_body(in_ref, out_ref, held):
    packed = unpack_rows(in_ref, held)
    for peer in range(out_ref.shape[0]):
        out_ref[peer] = packed


def ffn_body(in_ref, gate_ref, up_ref, down_ref, out_ref, wait):
    parts, rows, width = in_ref.shape
    total = jnp.zeros((rows, 2 * width), F32)
    for k in range(0, parts, 2):
        left = jnp.concatenate([in_ref[k], in_ref[k + 1]], axis=1)
        span = pl.ds(k * width, 2 * width)
        right = jnp.concatenate([gate_ref[span, :], up_ref[span, :]], axis=1)
        total = total + dot(left, right)
    hidden = (silu(total[:, :width]) * total[:, width:]).astype(BF16)
    wait()
    for k in range(0, parts, 2):
        value = dot(hidden, down_ref[:, k * width : (k + 2) * width]).astype(BF16)
        out_ref[k] = value[:, :width]
        out_ref[k + 1] = value[:, width:]


def sum_of(in_ref):
    total = in_ref[0].astype(F32)
    for k in range(1, in_ref.shape[0]):
        total = total + in_ref[k].astype(F32)
    return total.astype(BF16)


def expert_sum_body(in_ref, out_ref, held):
    pack_rows(sum_of(in_ref), held, out_ref)


def sum_body(in_ref, out_ref):
    out_ref[...] = sum_of(in_ref)


def combine_body(table_ref, routing_ref, score_ref, out_ref, held):
    tokens = routing_ref.shape[1]
    scores = upright(score_ref)
    whole = scores[:, 0:1] + scores[:, 1:2]
    table = unpack_rows(table_ref, held)
    place = iota((tokens, table.shape[0]), 1)
    total = jnp.zeros(out_ref.shape, F32)
    for index, slot in enumerate(slots_of(routing_ref, table_ref.shape[0])):
        pick = jnp.where(place == slot, 1.0, 0.0).astype(BF16)
        total = total + scores[:, index : index + 1] / whole * dot(pick, table)
    out_ref[...] = total.astype(BF16)


def conv_silu(values_ref, prior_ref, taps_ref, start, held):
    length = values_ref.shape[0]
    reach = taps_ref.shape[0] - 1
    held[0:8, :] = prior_ref[start : start + 8, :].astype(F32)
    held[8 : 8 + length, :] = values_ref[...].astype(F32)
    total = jnp.zeros(values_ref.shape, F32)
    for k in range(reach + 1):
        total = total + held[8 - reach + k : 8 - reach + k + length, :] * taps_ref[
            k : k + 1, :
        ].astype(F32)
    return silu(total).astype(BF16)


def running_sum(values):
    length = values.shape[0]
    reach = 1
    row = iota(values.shape, 0)
    while reach < length:
        moved = pltpu.roll(values, reach, 0)
        values = values + jnp.where(row >= reach, moved, 0.0)
        reach *= 2
    return values


def pair(left, right, dims, dim):
    return jnp.where(iota(dims, dim) < HEAD_DIM, left, right)


def block_terms(block, step_all, log_all):
    rows = slice(block * BLOCK, (block + 1) * BLOCK)
    step = step_all[rows]
    decay = running_sum(log_all[rows])
    return rows, step, decay, decay[BLOCK - 1 : BLOCK, :]


def states_body(
    x_ref, b_ref, c_ref, prior_ref, xt_ref, bt_ref, ct_ref, step_ref, extra_ref, rate_ref,
    xo_ref, bo_ref, co_ref, first_ref, total_ref, held, wide_ref,
):
    xo_ref[...] = conv_silu(x_ref, prior_ref, xt_ref, 0, held)
    bo_ref[...] = conv_silu(b_ref, prior_ref, bt_ref, 8, held)
    co_ref[...] = conv_silu(c_ref, prior_ref, ct_ref, 16, held)
    step_all, log_all = log_decay_of(step_ref, extra_ref, rate_ref)
    wide = (BLOCK, 128)
    for group in range(x_ref.shape[1] // 128):
        columns = slice(group * 128, (group + 1) * 128)
        a, b = 2 * group, 2 * group + 1
        state = None
        for block in range(x_ref.shape[0] // BLOCK):
            rows, step, decay, last = block_terms(block, step_all, log_all)
            x = xo_ref[rows, columns].astype(F32)
            x_step = (x * pair(step[:, a : a + 1], step[:, b : b + 1], wide, 1)).astype(BF16)
            left = jnp.exp(last - decay)
            weighted = x_step.astype(F32) * pair(left[:, a : a + 1], left[:, b : b + 1], wide, 1)
            new = dot(weighted.astype(BF16), bo_ref[rows, columns], 0, 0)
            if state is None:
                first_ref[columns, :] = new
                state = new
            else:
                kept = jnp.exp(last)
                state = state * pair(kept[:, a : a + 1], kept[:, b : b + 1], wide, 0) + new
        total_ref[columns, :] = state.astype(BF16)
    write_log(total_ref, jnp.sum(log_all, axis=0, keepdims=True), wide_ref)


def write_log(ref, log, wide_ref):
    rows = ref.shape[0] - NOTE
    wide_ref[...] = jnp.zeros_like(wide_ref)
    for part in range(3):
        piece = log.astype(ref.dtype).astype(F32)
        wide_ref[part : part + 1, 0 : log.shape[1]] = piece
        log = log - piece
    ref[rows:, :] = wide_ref[...].astype(ref.dtype)


def by_row(values, rows):
    head = iota((rows, 128), 0) // HEAD_DIM
    total = jnp.broadcast_to(values[:, 0:1], (rows, 128))
    for k in range(1, values.shape[1]):
        total = jnp.where(head == k, values[:, k : k + 1], total)
    return total


def read(part):
    rows = part.shape[0] - NOTE
    note = part[rows:, :].astype(F32)
    log = (note[0:1] + note[1:2] + note[2:3])[:, : rows // HEAD_DIM]
    return part[:rows, :].astype(F32), log


def joined(earlier, later):
    decay = by_row(jnp.exp(later[1]), later[0].shape[0])
    return earlier[0] * decay + later[0], earlier[1] + later[1]


def write(ref, value, wide_ref):
    ref[: ref.shape[0] - NOTE, :] = value[0].astype(ref.dtype)
    write_log(ref, value[1], wide_ref)


def read_half(both_ref, k):
    half = (both_ref.shape[1] - NOTE) // 2
    core = lax.axis_index("core")
    state = both_ref[k, pl.ds(pl.multiple_of(core * half, half), half), :].astype(F32)
    _, log = read(both_ref[k])
    heads = log.shape[1] // 2
    return state, jnp.where(core == 0, log[:, :heads], log[:, heads:])


def join_core_body(both_ref, out_ref, wide_ref):
    write(out_ref, joined(read_half(both_ref, 0), read_half(both_ref, 1)), wide_ref)


def join_first_body(came_ref, own_ref, out_ref, wide_ref):
    write(out_ref, joined(read(came_ref[...]), read(own_ref[...])), wide_ref)


def join_body(came_ref, own_ref, before_ref, out_ref, new_ref, wide_ref):
    came = read(came_ref[...])
    write(out_ref, joined(came, read(own_ref[...])), wide_ref)
    write(new_ref, joined(came, read(before_ref[...])), wide_ref)


def join_last_body(came_ref, before_ref, out_ref):
    out_ref[...] = joined(read(came_ref[...]), read(before_ref[...]))[0]


def income_of(chips_ref, both_ref):
    state = chips_ref[...]
    inside, _ = joined((state, 0.0), read(both_ref[0]))
    return jnp.where(lax.axis_index("core") == 1, inside, state)


def mixer_body(
    x_ref, b_ref, c_ref, gate_ref, first_ref, chips_ref, both_ref, step_ref, extra_ref,
    rate_ref, skip_ref, gain_ref, weight_ref, out_ref, normed, income_ref,
):
    income_ref[...] = income_of(chips_ref, both_ref)
    step_all, log_all = log_decay_of(step_ref, extra_ref, rate_ref)
    wide = (BLOCK, 128)
    causal = iota(wide, 0) >= iota(wide, 1)
    for block in range(x_ref.shape[0] // BLOCK):
        rows, step, decay, last = block_terms(block, step_all, log_all)
        grown = jnp.exp(decay)
        for group in range(x_ref.shape[1] // 128):
            columns = slice(group * 128, (group + 1) * 128)
            a, b = 2 * group, 2 * group + 1
            x = x_ref[rows, columns].astype(F32)
            x_step = (x * pair(step[:, a : a + 1], step[:, b : b + 1], wide, 1)).astype(BF16)
            c = c_ref[rows, columns]
            inner = dot(c, b_ref[rows, columns], 1, 1)
            parts = []
            for head in (a, b):
                along = jnp.broadcast_to(decay[:, head : head + 1], wide)
                distance = along - along.T
                scale = jnp.where(causal, jnp.exp(jnp.where(causal, distance, 0.0)), 0.0)
                parts.append(dot((inner * scale).astype(BF16), x_step))
            y = pair(parts[0], parts[1], wide, 1)
            entering = income_ref[columns, :]
            if block > 0:
                entering = entering * pair(kept[:, a : a + 1], kept[:, b : b + 1], wide, 0)
                entering = entering + first_ref[columns, :]
            off = dot(c, entering.astype(BF16), 1, 1)
            off = off * pair(grown[:, a : a + 1], grown[:, b : b + 1], wide, 1)
            skip = pair(skip_ref[:, a : a + 1], skip_ref[:, b : b + 1], wide, 1)
            mixed = (y + off + skip * x) * silu(gate_ref[rows, columns].astype(F32))
            mean = jnp.sum(mixed * mixed, axis=1, keepdims=True) * (1.0 / 128)
            mixed = mixed * lax.rsqrt(mean + eps) * gain_ref[:, columns]
            normed[rows, columns] = mixed.astype(BF16)
        kept = jnp.exp(last)
    for k in range(0, out_ref.shape[0], 2):
        value = dot(normed[...], weight_ref[:, k * 128 : (k + 2) * 128]).astype(BF16)
        out_ref[k] = value[:, :128]
        out_ref[k + 1] = value[:, 128:]


def all_to_all(value, axis):
    return lax.all_to_all(value, axis, split_axis=0, concat_axis=0, tiled=True)


def per_device(
    mixer_input_channels,
    input_state_projection,
    output_state_projection,
    output_gate_logits,
    step_size_logits,
    extra_log_decay,
    mixer_channel_taps,
    input_state_taps,
    output_state_taps,
    decay_rate_log,
    head_skip_weight,
    grouped_norm_gain,
    mixer_output_weight,
    expert_input_tokens,
    routing,
    router_chosen_scores,
    expert_norm_gain,
    expert_gate_weight,
    expert_up_weight,
    expert_down_weight,
):
    parts = lax.axis_size("tp")
    devices = lax.axis_size(EP)
    length, channels = mixer_input_channels.shape
    tokens, model = expert_input_tokens.shape
    top = routing.shape[1]
    capacity = (tokens * top * 5 + 4 * devices - 1) // (4 * devices)
    message = (devices, PACK, capacity // PACK * LANES)
    folded = pltpu.VMEM((devices * PACK, message[2]), BF16)
    slots = devices * capacity
    rate, skip = decay_rate_log[None], head_skip_weight[None]
    step_rows, extra_rows = step_size_logits.T, extra_log_decay.T
    routing_rows = routing.T

    outgoing, edge = kernel_call(
        dispatch_body,
        [shape(message, BF16), shape((24, channels), BF16)],
        (
            expert_input_tokens, expert_norm_gain[None], routing_rows,
            mixer_input_channels, input_state_projection, output_state_projection,
        ),
        2 * slots * tokens * 128,
        [folded],
        far=(0, 1, 2, 3, 4, 5),
        tails=(3, 4, 5),
        vmem=WHOLE_VMEM,
    )
    prior = lax.ppermute(edge, EP, [(i, i + 1) for i in range(devices - 1)])
    arrived = all_to_all(outgoing, EP)

    note = channels + NOTE
    wide = pltpu.VMEM((NOTE, 128), F32)
    x_conv, b_conv, c_conv, first, total = kernel_call(
        states_body,
        [shape((length, channels), BF16)] * 3
        + [shape((channels, STATE), F32), shape((note, STATE), BF16)],
        (
            mixer_input_channels, input_state_projection, output_state_projection, prior,
            mixer_channel_taps, input_state_taps, output_state_taps,
            step_rows, extra_rows, rate,
        ),
        2 * length * channels * STATE,
        [pltpu.VMEM((length + 8, channels), F32), wide],
        far=(0, 1, 2, 4, 5, 6, 7, 8, 9),
        vmem=WHOLE_VMEM,
    )

    def moved(value, distance):
        chips = lax.axis_size(CHIPS)
        route = [(i, i + distance) for i in range(chips - distance)]
        return lax.ppermute(value, CHIPS, route)

    half = channels // 2
    carried = shape((half + NOTE, STATE), BF16)

    def join(body, values, more=()):
        outs = [carried, *more]
        return kernel_call(body, outs, values, 4 * channels * STATE, [wide])

    both = lax.all_gather(total, "core")
    (upto,) = join(join_core_body, (both,))
    before = came = moved(upto, 1)
    (upto,) = join(join_first_body, (came, upto))
    for distance in (2, 4):
        came = moved(upto, distance)
        upto, before = join(join_body, (came, upto, before), [shape(carried.shape, F32)])
    (chips,) = kernel_call(
        join_last_body, [shape((half, STATE), F32)], (moved(upto, 8), before), 4 * half * STATE
    )
    chips = lax.all_gather(chips, "core", tiled=True)

    (copies,) = kernel_call(
        spread_body,
        [shape((parts, devices * capacity, 128), BF16)],
        (arrived,),
        parts * slots * 128,
        [folded],
    )
    gathered = all_to_all(copies, "tp")

    (partial_rows,) = kernel_call(
        ffn_body,
        [shape((parts, devices * capacity, 128), BF16)],
        (gathered, expert_gate_weight[0], expert_up_weight[0], expert_down_weight[0]),
        6 * devices * capacity * model * 128,
        far=(3,),
        late=(3,),
    )
    expert_parts = all_to_all(partial_rows, "tp")

    (mixer_part,) = kernel_call(
        mixer_body,
        [shape((parts, length, 128), BF16)],
        (
            x_conv, b_conv, c_conv, output_gate_logits, first, chips, both,
            step_rows, extra_rows, rate, skip, grouped_norm_gain[None], mixer_output_weight,
        ),
        2 * length * channels * model,
        [pltpu.VMEM((length, channels), BF16), pltpu.VMEM((channels, STATE), F32)],
    )
    mixer_parts = all_to_all(mixer_part, "tp")

    (back,) = kernel_call(
        expert_sum_body, [shape(message, BF16)], (expert_parts,), parts * slots * 128, [folded]
    )
    table = all_to_all(back, EP)

    (mixer_output_first,) = kernel_call(
        sum_body, [shape((length, 128), BF16)], (mixer_parts,), parts * length * 128
    )
    (moe_out,) = kernel_call(
        combine_body,
        [shape((tokens, 128), BF16)],
        (table, routing_rows, router_chosen_scores.T),
        4 * tokens * slots * 128,
        [folded],
    )
    return (mixer_output_first, moe_out)


def solution(mesh):
    split = Mesh(mesh.devices.reshape(16, 2, mesh.shape["tp"]), (*EP, "tp"))
    in_specs = (
        P(EP, "tp"),
        P(EP, "tp"),
        P(EP, "tp"),
        P(EP, "tp"),
        P(EP, "tp"),
        P(EP, "tp"),
        P(None, "tp"),
        P(None, "tp"),
        P(None, "tp"),
        P("tp"),
        P("tp"),
        P("tp"),
        P("tp", None),
        P(EP, None),
        P(EP, None),
        P(EP, None),
        P(),
        P(EP, None, "tp"),
        P(EP, None, "tp"),
        P(EP, "tp", None),
    )
    out_specs = (P(EP, "tp"), P(EP, "tp"))
    return jax.shard_map(
        per_device, mesh=split, in_specs=in_specs, out_specs=out_specs, check_vma=False
    )
```

```python
import jax
import jax.numpy as jnp
from jax import lax
from jax.experimental import pallas as pl
from jax.experimental.pallas import tpu as pltpu
from jax.sharding import Mesh
from jax.sharding import PartitionSpec as P

HEAD_DIM = 64
STATE = 128
BLOCK = 128
CHIPS = ("ep_hi", "ep_lo")
EP = (*CHIPS, "core")
LANES = 128
PACK = 2
NOTE = 16
VMEM = 16 << 20
WHOLE_VMEM = 60 << 20
F32 = jnp.float32
BF16 = jnp.bfloat16

eps = 1e-06


def iota(shape, dim):
    return lax.broadcasted_iota(jnp.int32, shape, dim)


def dot(a, b, ca=1, cb=0, precision=None):
    return lax.dot_general(
        a, b, (((ca,), (cb,)), ((), ())), precision=precision, preferred_element_type=F32
    )


def silu(x):
    return x * (1.0 / (1.0 + jnp.exp(-x)))


def softplus(x):
    return jnp.maximum(x, 0.0) + jnp.log1p(jnp.exp(-jnp.abs(x)))


def fetched(body, ins, outs, own, far, late):
    def whole(*refs):
        given, rest = list(refs[:ins]), refs[ins : ins + outs + own]
        held, sems = refs[ins + outs + own : -1], refs[-1]
        copies = {}
        for k, index in enumerate(far):
            source = given[index]
            if source.shape != held[k].shape:
                source = source.at[pl.ds(source.shape[0] - held[k].shape[0], held[k].shape[0]), :]
            copies[index] = pltpu.make_async_copy(source, held[k], sems.at[k])
            copies[index].start()
            given[index] = held[k]
        for index in far:
            if index not in late:
                copies[index].wait()
        body(*given, *rest, *(copies[index].wait for index in late))

    return whole


def kernel_call(body, outs, args, flops, scratch=(), far=(), late=(), tails=(), vmem=VMEM):
    size = sum(a.size * a.dtype.itemsize for a in args)
    size += sum(o.size * o.dtype.itemsize for o in outs)
    specs = [
        pl.BlockSpec(memory_space=pltpu.HBM if k in far else pltpu.VMEM) for k in range(len(args))
    ]
    scratch = list(scratch)
    if far:
        body = fetched(body, len(args), len(outs), len(scratch), far, late)
        for k in far:
            dims = (8, args[k].shape[1]) if k in tails else args[k].shape
            scratch.append(pltpu.VMEM(dims, args[k].dtype))
        scratch.append(pltpu.SemaphoreType.DMA((len(far),)))
    return pl.pallas_call(
        body,
        out_shape=outs,
        in_specs=specs,
        out_specs=[pl.BlockSpec(memory_space=pltpu.VMEM)] * len(outs),
        scratch_shapes=scratch,
        cost_estimate=pl.CostEstimate(flops=flops, bytes_accessed=size, transcendentals=0),
        compiler_params=pltpu.CompilerParams(vmem_limit_bytes=vmem),
    )(*args)


def shape(dims, kind):
    return jax.ShapeDtypeStruct(dims, kind)


def upright(ref):
    wide = jnp.concatenate([ref[...].astype(F32)] * (8 // ref.shape[0]), axis=0)
    return wide.T[:, : ref.shape[0]]


def slots_of(routing_ref, experts):
    tokens = routing_ref.shape[1]
    expert = iota((tokens, 128), 1)
    named = upright(routing_ref).astype(jnp.int32)
    first = expert == named[:, 0:1]
    second = expert == named[:, 1:2]
    member = jnp.where(first | second, 1.0, 0.0).astype(BF16)
    earlier = jnp.where(iota((tokens, tokens), 0) > iota((tokens, tokens), 1), 1.0, 0.0)
    place = dot(earlier.astype(BF16), member)
    slots = []
    for index, chosen in enumerate((first, second)):
        rank = jnp.sum(jnp.where(chosen, place, 0.0), axis=1, keepdims=True).astype(jnp.int32)
        number = named[:, index : index + 1] * PACK + rank % PACK
        slots.append(rank // PACK * (PACK * experts) + number)
    return slots


def pack_rows(rows, held, out_ref):
    experts = out_ref.shape[0]
    span = PACK * experts
    for k in range(out_ref.shape[2] // LANES):
        held[:, k * LANES : (k + 1) * LANES] = rows[k * span : (k + 1) * span, :]
    for e in range(experts):
        out_ref[e] = held[PACK * e : PACK * (e + 1), :]


def unpack_rows(in_ref, held):
    for e in range(in_ref.shape[0]):
        held[PACK * e : PACK * (e + 1), :] = in_ref[e]
    parts = [held[:, k : k + LANES] for k in range(0, in_ref.shape[2], LANES)]
    return jnp.concatenate(parts, axis=0)


def log_decay_of(step_ref, extra_ref, rate_ref):
    step = softplus(upright(step_ref))
    return step, step * -jnp.exp(rate_ref[...]) + upright(extra_ref)


def dispatch_body(
    tok_ref, gain_ref, routing_ref, x_ref, b_ref, c_ref, out_ref, edge_ref, held
):
    tokens, model = tok_ref.shape
    rows = tok_ref[...].astype(F32)
    scale = lax.rsqrt(jnp.sum(rows * rows, axis=1, keepdims=True) * (1.0 / model) + eps)
    columns = pl.ds(pl.multiple_of(lax.axis_index("tp") * 128, 128), 128)
    own = (tok_ref[:, columns].astype(F32) * scale * gain_ref[:, columns]).astype(BF16)
    experts = out_ref.shape[0]
    slots = slots_of(routing_ref, experts)
    place = iota((tokens, out_ref.shape[1] * experts * out_ref.shape[2] // LANES), 1)
    pick = jnp.where((place == slots[0]) | (place == slots[1]), 1.0, 0.0).astype(BF16)
    pack_rows(dot(pick, own, 0, 0).astype(BF16), held, out_ref)
    for k, ref in enumerate((x_ref, b_ref, c_ref)):
        edge_ref[8 * k : 8 * k + 8, :] = ref[...]


def spread_body(in_ref, out_ref, held):
    packed = unpack_rows(in_ref, held)
    for peer in range(out_ref.shape[0]):
        out_ref[peer] = packed


def ffn_body(in_ref, gate_ref, up_ref, down_ref, out_ref, wait):
    parts, rows, width = in_ref.shape
    total = jnp.zeros((rows, 2 * width), F32)
    for k in range(0, parts, 2):
        left = jnp.concatenate([in_ref[k], in_ref[k + 1]], axis=1)
        span = pl.ds(k * width, 2 * width)
        right = jnp.concatenate([gate_ref[span, :], up_ref[span, :]], axis=1)
        total = total + dot(left, right)
    hidden = (silu(total[:, :width]) * total[:, width:]).astype(BF16)
    wait()
    for k in range(0, parts, 2):
        value = dot(hidden, down_ref[:, k * width : (k + 2) * width]).astype(BF16)
        out_ref[k] = value[:, :width]
        out_ref[k + 1] = value[:, width:]


def sum_of(in_ref):
    total = in_ref[0].astype(F32)
    for k in range(1, in_ref.shape[0]):
        total = total + in_ref[k].astype(F32)
    return total.astype(BF16)


def expert_sum_body(in_ref, out_ref, held):
    pack_rows(sum_of(in_ref), held, out_ref)


def sum_body(in_ref, out_ref):
    out_ref[...] = sum_of(in_ref)


def combine_body(table_ref, routing_ref, score_ref, out_ref, held):
    tokens = routing_ref.shape[1]
    scores = upright(score_ref)
    whole = scores[:, 0:1] + scores[:, 1:2]
    table = unpack_rows(table_ref, held)
    place = iota((tokens, table.shape[0]), 1)
    total = jnp.zeros(out_ref.shape, F32)
    for index, slot in enumerate(slots_of(routing_ref, table_ref.shape[0])):
        pick = jnp.where(place == slot, 1.0, 0.0).astype(BF16)
        total = total + scores[:, index : index + 1] / whole * dot(pick, table)
    out_ref[...] = total.astype(BF16)


def conv_silu(values_ref, prior_ref, taps_ref, start, held):
    length = values_ref.shape[0]
    reach = taps_ref.shape[0] - 1
    held[0:8, :] = prior_ref[start : start + 8, :].astype(F32)
    held[8 : 8 + length, :] = values_ref[...].astype(F32)
    total = jnp.zeros(values_ref.shape, F32)
    for k in range(reach + 1):
        total = total + held[8 - reach + k : 8 - reach + k + length, :] * taps_ref[
            k : k + 1, :
        ].astype(F32)
    return silu(total).astype(BF16)


def running_sum(values):
    length = values.shape[0]
    reach = 1
    row = iota(values.shape, 0)
    while reach < length:
        moved = pltpu.roll(values, reach, 0)
        values = values + jnp.where(row >= reach, moved, 0.0)
        reach *= 2
    return values


def pair(left, right, dims, dim):
    return jnp.where(iota(dims, dim) < HEAD_DIM, left, right)


def block_terms(block, step_all, log_all):
    rows = slice(block * BLOCK, (block + 1) * BLOCK)
    step = step_all[rows]
    decay = running_sum(log_all[rows])
    return rows, step, decay, decay[BLOCK - 1 : BLOCK, :]


def states_body(
    x_ref, b_ref, c_ref, prior_ref, xt_ref, bt_ref, ct_ref, step_ref, extra_ref, rate_ref,
    xo_ref, bo_ref, co_ref, first_ref, total_ref, held, wide_ref,
):
    xo_ref[...] = conv_silu(x_ref, prior_ref, xt_ref, 0, held)
    bo_ref[...] = conv_silu(b_ref, prior_ref, bt_ref, 8, held)
    co_ref[...] = conv_silu(c_ref, prior_ref, ct_ref, 16, held)
    step_all, log_all = log_decay_of(step_ref, extra_ref, rate_ref)
    wide = (BLOCK, 128)
    for group in range(x_ref.shape[1] // 128):
        columns = slice(group * 128, (group + 1) * 128)
        a, b = 2 * group, 2 * group + 1
        state = None
        for block in range(x_ref.shape[0] // BLOCK):
            rows, step, decay, last = block_terms(block, step_all, log_all)
            x = xo_ref[rows, columns].astype(F32)
            x_step = (x * pair(step[:, a : a + 1], step[:, b : b + 1], wide, 1)).astype(BF16)
            left = jnp.exp(last - decay)
            weighted = x_step.astype(F32) * pair(left[:, a : a + 1], left[:, b : b + 1], wide, 1)
            new = dot(weighted.astype(BF16), bo_ref[rows, columns], 0, 0)
            if state is None:
                first_ref[columns, :] = new
                state = new
            else:
                kept = jnp.exp(last)
                state = state * pair(kept[:, a : a + 1], kept[:, b : b + 1], wide, 0) + new
        total_ref[columns, :] = state.astype(BF16)
    write_log(total_ref, jnp.sum(log_all, axis=0, keepdims=True), wide_ref)


def write_log(ref, log, wide_ref):
    rows = ref.shape[0] - NOTE
    wide_ref[...] = jnp.zeros_like(wide_ref)
    for part in range(3):
        piece = log.astype(ref.dtype).astype(F32)
        wide_ref[part : part + 1, 0 : log.shape[1]] = piece
        log = log - piece
    ref[rows:, :] = wide_ref[...].astype(ref.dtype)


def by_row(values, rows):
    head = iota((rows, 128), 0) // HEAD_DIM
    total = jnp.broadcast_to(values[:, 0:1], (rows, 128))
    for k in range(1, values.shape[1]):
        total = jnp.where(head == k, values[:, k : k + 1], total)
    return total


def read(part):
    rows = part.shape[0] - NOTE
    note = part[rows:, :].astype(F32)
    log = (note[0:1] + note[1:2] + note[2:3])[:, : rows // HEAD_DIM]
    return part[:rows, :].astype(F32), log


def joined(earlier, later):
    decay = by_row(jnp.exp(later[1]), later[0].shape[0])
    return earlier[0] * decay + later[0], earlier[1] + later[1]


def write(ref, value, wide_ref):
    ref[: ref.shape[0] - NOTE, :] = value[0].astype(ref.dtype)
    write_log(ref, value[1], wide_ref)


def read_half(both_ref, k):
    half = (both_ref.shape[1] - NOTE) // 2
    core = lax.axis_index("core")
    state = both_ref[k, pl.ds(pl.multiple_of(core * half, half), half), :].astype(F32)
    _, log = read(both_ref[k])
    heads = log.shape[1] // 2
    return state, jnp.where(core == 0, log[:, :heads], log[:, heads:])


def join_core_body(both_ref, out_ref, wide_ref):
    write(out_ref, joined(read_half(both_ref, 0), read_half(both_ref, 1)), wide_ref)


def join_first_body(came_ref, own_ref, out_ref, wide_ref):
    write(out_ref, joined(read(came_ref[...]), read(own_ref[...])), wide_ref)


def join_body(came_ref, own_ref, before_ref, out_ref, new_ref, wide_ref):
    came = read(came_ref[...])
    write(out_ref, joined(came, read(own_ref[...])), wide_ref)
    write(new_ref, joined(came, read(before_ref[...])), wide_ref)


def join_far_body(far_ref, before_ref, out_ref):
    rows = far_ref.shape[1] - NOTE
    me = lax.axis_index(CHIPS[0])
    state = jnp.zeros((rows, 128), F32)
    for k in range(far_ref.shape[0] - 1):
        state = jnp.where(k < me, joined((state, 0.0), read(far_ref[k]))[0], state)
    out_ref[...] = joined((state, 0.0), read(before_ref[...]))[0]


def income_of(chips_ref, both_ref):
    state = chips_ref[...]
    inside, _ = joined((state, 0.0), read(both_ref[0]))
    return jnp.where(lax.axis_index("core") == 1, inside, state)


def mixer_body(
    x_ref, b_ref, c_ref, gate_ref, first_ref, chips_ref, both_ref, step_ref, extra_ref,
    rate_ref, skip_ref, gain_ref, weight_ref, out_ref, normed, income_ref,
):
    income_ref[...] = income_of(chips_ref, both_ref)
    step_all, log_all = log_decay_of(step_ref, extra_ref, rate_ref)
    wide = (BLOCK, 128)
    causal = iota(wide, 0) >= iota(wide, 1)
    for block in range(x_ref.shape[0] // BLOCK):
        rows, step, decay, last = block_terms(block, step_all, log_all)
        grown = jnp.exp(decay)
        for group in range(x_ref.shape[1] // 128):
            columns = slice(group * 128, (group + 1) * 128)
            a, b = 2 * group, 2 * group + 1
            x = x_ref[rows, columns].astype(F32)
            x_step = (x * pair(step[:, a : a + 1], step[:, b : b + 1], wide, 1)).astype(BF16)
            c = c_ref[rows, columns]
            inner = dot(c, b_ref[rows, columns], 1, 1)
            parts = []
            for head in (a, b):
                along = jnp.broadcast_to(decay[:, head : head + 1], wide)
                distance = along - along.T
                scale = jnp.where(causal, jnp.exp(jnp.where(causal, distance, 0.0)), 0.0)
                parts.append(dot((inner * scale).astype(BF16), x_step))
            y = pair(parts[0], parts[1], wide, 1)
            entering = income_ref[columns, :]
            if block > 0:
                entering = entering * pair(kept[:, a : a + 1], kept[:, b : b + 1], wide, 0)
                entering = entering + first_ref[columns, :]
            off = dot(c, entering.astype(BF16), 1, 1)
            off = off * pair(grown[:, a : a + 1], grown[:, b : b + 1], wide, 1)
            skip = pair(skip_ref[:, a : a + 1], skip_ref[:, b : b + 1], wide, 1)
            mixed = (y + off + skip * x) * silu(gate_ref[rows, columns].astype(F32))
            mean = jnp.sum(mixed * mixed, axis=1, keepdims=True) * (1.0 / 128)
            mixed = mixed * lax.rsqrt(mean + eps) * gain_ref[:, columns]
            normed[rows, columns] = mixed.astype(BF16)
        kept = jnp.exp(last)
    for k in range(0, out_ref.shape[0], 2):
        value = dot(normed[...], weight_ref[:, k * 128 : (k + 2) * 128]).astype(BF16)
        out_ref[k] = value[:, :128]
        out_ref[k + 1] = value[:, 128:]


def all_to_all(value, axis):
    return lax.all_to_all(value, axis, split_axis=0, concat_axis=0, tiled=True)


def per_device(
    mixer_input_channels,
    input_state_projection,
    output_state_projection,
    output_gate_logits,
    step_size_logits,
    extra_log_decay,
    mixer_channel_taps,
    input_state_taps,
    output_state_taps,
    decay_rate_log,
    head_skip_weight,
    grouped_norm_gain,
    mixer_output_weight,
    expert_input_tokens,
    routing,
    router_chosen_scores,
    expert_norm_gain,
    expert_gate_weight,
    expert_up_weight,
    expert_down_weight,
):
    parts = lax.axis_size("tp")
    devices = lax.axis_size(EP)
    length, channels = mixer_input_channels.shape
    tokens, model = expert_input_tokens.shape
    top = routing.shape[1]
    capacity = (tokens * top * 5 + 4 * devices - 1) // (4 * devices)
    message = (devices, PACK, capacity // PACK * LANES)
    folded = pltpu.VMEM((devices * PACK, message[2]), BF16)
    slots = devices * capacity
    rate, skip = decay_rate_log[None], head_skip_weight[None]
    step_rows, extra_rows = step_size_logits.T, extra_log_decay.T
    routing_rows = routing.T

    outgoing, edge = kernel_call(
        dispatch_body,
        [shape(message, BF16), shape((24, channels), BF16)],
        (
            expert_input_tokens, expert_norm_gain[None], routing_rows,
            mixer_input_channels, input_state_projection, output_state_projection,
        ),
        2 * slots * tokens * 128,
        [folded],
        far=(0, 1, 2, 3, 4, 5),
        tails=(3, 4, 5),
        vmem=WHOLE_VMEM,
    )
    prior = lax.ppermute(edge, EP, [(i, i + 1) for i in range(devices - 1)])
    arrived = all_to_all(outgoing, EP)

    note = channels + NOTE
    wide = pltpu.VMEM((NOTE, 128), F32)
    x_conv, b_conv, c_conv, first, total = kernel_call(
        states_body,
        [shape((length, channels), BF16)] * 3
        + [shape((channels, STATE), F32), shape((note, STATE), BF16)],
        (
            mixer_input_channels, input_state_projection, output_state_projection, prior,
            mixer_channel_taps, input_state_taps, output_state_taps,
            step_rows, extra_rows, rate,
        ),
        2 * length * channels * STATE,
        [pltpu.VMEM((length + 8, channels), F32), wide],
        far=(0, 1, 2, 4, 5, 6, 7, 8, 9),
        vmem=WHOLE_VMEM,
    )

    def moved(value, distance):
        chips = lax.axis_size(CHIPS)
        route = [(i, i + distance) for i in range(chips - distance)]
        return lax.ppermute(value, CHIPS, route)

    half = channels // 2
    carried = shape((half + NOTE, STATE), BF16)

    def join(body, values, more=()):
        outs = [carried, *more]
        return kernel_call(body, outs, values, 4 * channels * STATE, [wide])

    both = lax.all_gather(total, "core")
    (upto,) = join(join_core_body, (both,))
    before = came = moved(upto, 1)
    (upto,) = join(join_first_body, (came, upto))
    upto, before = join(join_body, (moved(upto, 2), upto, before), [shape(carried.shape, F32)])
    far = lax.all_gather(upto, CHIPS[0])
    (chips,) = kernel_call(
        join_far_body, [shape((half, STATE), F32)], (far, before), 8 * half * STATE
    )
    chips = lax.all_gather(chips, "core", tiled=True)

    (copies,) = kernel_call(
        spread_body,
        [shape((parts, devices * capacity, 128), BF16)],
        (arrived,),
        parts * slots * 128,
        [folded],
    )
    gathered = all_to_all(copies, "tp")

    (partial_rows,) = kernel_call(
        ffn_body,
        [shape((parts, devices * capacity, 128), BF16)],
        (gathered, expert_gate_weight[0], expert_up_weight[0], expert_down_weight[0]),
        6 * devices * capacity * model * 128,
        far=(3,),
        late=(3,),
    )
    expert_parts = all_to_all(partial_rows, "tp")

    (mixer_part,) = kernel_call(
        mixer_body,
        [shape((parts, length, 128), BF16)],
        (
            x_conv, b_conv, c_conv, output_gate_logits, first, chips, both,
            step_rows, extra_rows, rate, skip, grouped_norm_gain[None], mixer_output_weight,
        ),
        2 * length * channels * model,
        [pltpu.VMEM((length, channels), BF16), pltpu.VMEM((channels, STATE), F32)],
    )
    mixer_parts = all_to_all(mixer_part, "tp")

    (back,) = kernel_call(
        expert_sum_body, [shape(message, BF16)], (expert_parts,), parts * slots * 128, [folded]
    )
    table = all_to_all(back, EP)

    (mixer_output_first,) = kernel_call(
        sum_body, [shape((length, 128), BF16)], (mixer_parts,), parts * length * 128
    )
    (moe_out,) = kernel_call(
        combine_body,
        [shape((tokens, 128), BF16)],
        (table, routing_rows, router_chosen_scores.T),
        4 * tokens * slots * 128,
        [folded],
    )
    return (mixer_output_first, moe_out)


def solution(mesh):
    split = Mesh(mesh.devices.reshape(4, 4, 2, mesh.shape["tp"]), (*EP, "tp"))
    in_specs = (
        P(EP, "tp"),
        P(EP, "tp"),
        P(EP, "tp"),
        P(EP, "tp"),
        P(EP, "tp"),
        P(EP, "tp"),
        P(None, "tp"),
        P(None, "tp"),
        P(None, "tp"),
        P("tp"),
        P("tp"),
        P("tp"),
        P("tp", None),
        P(EP, None),
        P(EP, None),
        P(EP, None),
        P(),
        P(EP, None, "tp"),
        P(EP, None, "tp"),
        P(EP, "tp", None),
    )
    out_specs = (P(EP, "tp"), P(EP, "tp"))
    return jax.shard_map(
        per_device, mesh=split, in_specs=in_specs, out_specs=out_specs, check_vma=False
    )
```

```python
import jax
import jax.numpy as jnp
from jax import lax
from jax.experimental import pallas as pl
from jax.experimental.pallas import tpu as pltpu
from jax.sharding import Mesh
from jax.sharding import PartitionSpec as P

HEAD_DIM = 64
STATE = 128
BLOCK = 128
EP = ("ep_hi", "ep_lo", "core")
LANES = 128
PACK = 2
NOTE = 16
VMEM = 16 << 20
WHOLE_VMEM = 60 << 20
F32 = jnp.float32
BF16 = jnp.bfloat16

eps = 1e-06


def iota(shape, dim):
    return lax.broadcasted_iota(jnp.int32, shape, dim)


def dot(a, b, ca=1, cb=0, precision=None):
    return lax.dot_general(
        a, b, (((ca,), (cb,)), ((), ())), precision=precision, preferred_element_type=F32
    )


def silu(x):
    return x * (1.0 / (1.0 + jnp.exp(-x)))


def softplus(x):
    return jnp.maximum(x, 0.0) + jnp.log1p(jnp.exp(-jnp.abs(x)))


def fetched(body, ins, outs, own, far, late):
    def whole(*refs):
        given, rest = list(refs[:ins]), refs[ins : ins + outs + own]
        held, sems = refs[ins + outs + own : -1], refs[-1]
        copies = {}
        for k, index in enumerate(far):
            source = given[index]
            if source.shape != held[k].shape:
                source = source.at[pl.ds(source.shape[0] - held[k].shape[0], held[k].shape[0]), :]
            copies[index] = pltpu.make_async_copy(source, held[k], sems.at[k])
            copies[index].start()
            given[index] = held[k]
        for index in far:
            if index not in late:
                copies[index].wait()
        body(*given, *rest, *(copies[index].wait for index in late))

    return whole


def kernel_call(body, outs, args, flops, scratch=(), far=(), late=(), tails=(), vmem=VMEM, out=None):
    out = out or [pltpu.VMEM] * len(outs)
    size = sum(a.size * a.dtype.itemsize for a in args)
    size += sum(o.size * o.dtype.itemsize for o in outs)
    specs = [
        pl.BlockSpec(memory_space=pltpu.HBM if k in far else pltpu.VMEM) for k in range(len(args))
    ]
    scratch = list(scratch)
    if far:
        body = fetched(body, len(args), len(outs), len(scratch), far, late)
        for k in far:
            dims = (8, args[k].shape[1]) if k in tails else args[k].shape
            scratch.append(pltpu.VMEM(dims, args[k].dtype))
        scratch.append(pltpu.SemaphoreType.DMA((len(far),)))
    return pl.pallas_call(
        body,
        out_shape=outs,
        in_specs=specs,
        out_specs=[pl.BlockSpec(memory_space=kind) for kind in out],
        scratch_shapes=scratch,
        cost_estimate=pl.CostEstimate(flops=flops, bytes_accessed=size, transcendentals=0),
        compiler_params=pltpu.CompilerParams(vmem_limit_bytes=vmem),
    )(*args)


def shape(dims, kind):
    return jax.ShapeDtypeStruct(dims, kind)


def upright(ref):
    wide = jnp.concatenate([ref[...].astype(F32)] * (8 // ref.shape[0]), axis=0)
    return wide.T[:, : ref.shape[0]]


def slots_of(routing_ref, experts):
    tokens = routing_ref.shape[1]
    expert = iota((tokens, 128), 1)
    named = upright(routing_ref).astype(jnp.int32)
    first = expert == named[:, 0:1]
    second = expert == named[:, 1:2]
    member = jnp.where(first | second, 1.0, 0.0).astype(BF16)
    earlier = jnp.where(iota((tokens, tokens), 0) > iota((tokens, tokens), 1), 1.0, 0.0)
    place = dot(earlier.astype(BF16), member)
    slots = []
    for index, chosen in enumerate((first, second)):
        rank = jnp.sum(jnp.where(chosen, place, 0.0), axis=1, keepdims=True).astype(jnp.int32)
        number = named[:, index : index + 1] * PACK + rank % PACK
        slots.append(rank // PACK * (PACK * experts) + number)
    return slots


def pack_rows(rows, held, out_ref):
    experts = out_ref.shape[0]
    span = PACK * experts
    for k in range(rows.shape[0] // span):
        held[:, k * LANES : (k + 1) * LANES] = rows[k * span : (k + 1) * span, :]
    for e in range(experts):
        out_ref[e] = held[PACK * e : PACK * (e + 1), :]


def unpack_rows(in_ref, held, width):
    for e in range(in_ref.shape[0]):
        held[PACK * e : PACK * (e + 1), :] = in_ref[e]
    parts = [held[:, k : k + LANES] for k in range(0, width, LANES)]
    return jnp.concatenate(parts, axis=0)


def log_decay_of(step_ref, extra_ref, rate_ref):
    step = softplus(upright(step_ref))
    return step, step * -jnp.exp(rate_ref[...]) + upright(extra_ref)


def dispatch_body(
    tok_ref, gain_ref, routing_ref, x_ref, b_ref, c_ref, step_ref, extra_ref, rate_ref,
    out_ref, edge_ref, held, wide_ref,
):
    tokens, model = tok_ref.shape
    rows = tok_ref[...].astype(F32)
    scale = lax.rsqrt(jnp.sum(rows * rows, axis=1, keepdims=True) * (1.0 / model) + eps)
    columns = pl.ds(pl.multiple_of(lax.axis_index("tp") * 128, 128), 128)
    own = (tok_ref[:, columns].astype(F32) * scale * gain_ref[:, columns]).astype(BF16)
    experts = out_ref.shape[0]
    width = out_ref.shape[2] - LANES
    _, log = log_decay_of(step_ref, extra_ref, rate_ref)
    log = jnp.sum(log, axis=0, keepdims=True)
    high = log.astype(BF16).astype(F32)
    wide_ref[...] = jnp.zeros_like(wide_ref)
    wide_ref[0:1, 0 : log.shape[1]] = high
    wide_ref[1:2, 0 : log.shape[1]] = log - high
    first = iota((experts * PACK, LANES), 0) % PACK == 0
    held[:, width:] = jnp.where(first, wide_ref[0:1, :], wide_ref[1:2, :]).astype(BF16)
    slots = slots_of(routing_ref, experts)
    place = iota((tokens, PACK * experts * width // LANES), 1)
    pick = jnp.where((place == slots[0]) | (place == slots[1]), 1.0, 0.0).astype(BF16)
    pack_rows(dot(pick, own, 0, 0).astype(BF16), held, out_ref)
    for k, ref in enumerate((x_ref, b_ref, c_ref)):
        edge_ref[8 * k : 8 * k + 8, :] = ref[...]


def spread_body(in_ref, out_ref, log_ref, held, packed, sems):
    width = in_ref.shape[2] - LANES
    packed[...] = unpack_rows(in_ref, held, width)
    log_ref[...] = held[:, width:]
    copies = [
        pltpu.make_async_copy(packed, out_ref.at[peer], sems.at[peer])
        for peer in range(out_ref.shape[0])
    ]
    for copy in copies:
        copy.start()
    for copy in copies:
        copy.wait()


def ffn_body(in_ref, gate_ref, up_ref, down_ref, out_ref, held, sems, wait):
    parts, rows, width = in_ref.shape
    total = jnp.zeros((rows, 2 * width), F32)
    for k in range(0, parts, 2):
        left = jnp.concatenate([in_ref[k], in_ref[k + 1]], axis=1)
        span = pl.ds(k * width, 2 * width)
        right = jnp.concatenate([gate_ref[span, :], up_ref[span, :]], axis=1)
        total = total + dot(left, right)
    hidden = (silu(total[:, :width]) * total[:, width:]).astype(BF16)
    wait()
    copies = []
    for k in range(0, parts, 2):
        value = dot(hidden, down_ref[:, k * width : (k + 2) * width]).astype(BF16)
        held[k] = value[:, :width]
        held[k + 1] = value[:, width:]
        if copies:
            copies[-1].start()
        both = pl.ds(k, 2)
        copies.append(pltpu.make_async_copy(held.at[both], out_ref.at[both], sems.at[k // 2]))
    copies[-1].start()
    for copy in copies:
        copy.wait()


def sum_of(in_ref):
    total = in_ref[0].astype(F32)
    for k in range(1, in_ref.shape[0]):
        total = total + in_ref[k].astype(F32)
    return total.astype(BF16)


def expert_sum_body(in_ref, out_ref, held):
    pack_rows(sum_of(in_ref), held, out_ref)


def sum_body(in_ref, out_ref):
    out_ref[...] = sum_of(in_ref)


def combine_body(table_ref, routing_ref, score_ref, out_ref, held):
    tokens = routing_ref.shape[1]
    scores = upright(score_ref)
    whole = scores[:, 0:1] + scores[:, 1:2]
    table = unpack_rows(table_ref, held, table_ref.shape[2])
    place = iota((tokens, table.shape[0]), 1)
    total = jnp.zeros(out_ref.shape, F32)
    for index, slot in enumerate(slots_of(routing_ref, table_ref.shape[0])):
        pick = jnp.where(place == slot, 1.0, 0.0).astype(BF16)
        total = total + scores[:, index : index + 1] / whole * dot(pick, table)
    out_ref[...] = total.astype(BF16)


def conv_silu(values_ref, prior_ref, taps_ref, start, held):
    length = values_ref.shape[0]
    reach = taps_ref.shape[0] - 1
    held[0:8, :] = prior_ref[start : start + 8, :].astype(F32)
    held[8 : 8 + length, :] = values_ref[...].astype(F32)
    total = jnp.zeros(values_ref.shape, F32)
    for k in range(reach + 1):
        total = total + held[8 - reach + k : 8 - reach + k + length, :] * taps_ref[
            k : k + 1, :
        ].astype(F32)
    return silu(total).astype(BF16)


def running_sum(values):
    length = values.shape[0]
    reach = 1
    row = iota(values.shape, 0)
    while reach < length:
        moved = pltpu.roll(values, reach, 0)
        values = values + jnp.where(row >= reach, moved, 0.0)
        reach *= 2
    return values


def pair(left, right, dims, dim):
    return jnp.where(iota(dims, dim) < HEAD_DIM, left, right)


def block_terms(block, step_all, log_all):
    rows = slice(block * BLOCK, (block + 1) * BLOCK)
    step = step_all[rows]
    decay = running_sum(log_all[rows])
    return rows, step, decay, decay[BLOCK - 1 : BLOCK, :]


def states_body(
    x_ref, b_ref, prior_ref, xt_ref, bt_ref, step_ref, extra_ref, rate_ref,
    xo_ref, bo_ref, first_ref, total_ref, held, wide_ref,
):
    xo_ref[...] = conv_silu(x_ref, prior_ref, xt_ref, 0, held)
    bo_ref[...] = conv_silu(b_ref, prior_ref, bt_ref, 8, held)
    step_all, log_all = log_decay_of(step_ref, extra_ref, rate_ref)
    wide = (BLOCK, 128)
    for group in range(x_ref.shape[1] // 128):
        columns = slice(group * 128, (group + 1) * 128)
        a, b = 2 * group, 2 * group + 1
        state = None
        for block in range(x_ref.shape[0] // BLOCK):
            rows, step, decay, last = block_terms(block, step_all, log_all)
            x = xo_ref[rows, columns].astype(F32)
            x_step = (x * pair(step[:, a : a + 1], step[:, b : b + 1], wide, 1)).astype(BF16)
            left = jnp.exp(last - decay)
            weighted = x_step.astype(F32) * pair(left[:, a : a + 1], left[:, b : b + 1], wide, 1)
            new = dot(weighted.astype(BF16), bo_ref[rows, columns], 0, 0)
            if state is None:
                first_ref[columns, :] = new
                state = new
            else:
                kept = jnp.exp(last)
                state = state * pair(kept[:, a : a + 1], kept[:, b : b + 1], wide, 0) + new
        total_ref[columns, :] = state.astype(BF16)
    write_log(total_ref, jnp.sum(log_all, axis=0, keepdims=True), wide_ref)


def write_log(ref, log, wide_ref):
    rows = ref.shape[0] - NOTE
    wide_ref[...] = jnp.zeros_like(wide_ref)
    for part in range(3):
        piece = log.astype(ref.dtype).astype(F32)
        wide_ref[part : part + 1, 0 : log.shape[1]] = piece
        log = log - piece
    ref[rows:, :] = wide_ref[...].astype(ref.dtype)


def by_row(values, rows):
    head = iota((rows, 128), 0) // HEAD_DIM
    total = jnp.broadcast_to(values[:, 0:1], (rows, 128))
    for k in range(1, values.shape[1]):
        total = jnp.where(head == k, values[:, k : k + 1], total)
    return total


def read(part):
    rows = part.shape[0] - NOTE
    note = part[rows:, :].astype(F32)
    log = (note[0:1] + note[1:2] + note[2:3])[:, : rows // HEAD_DIM]
    return part[:rows, :].astype(F32), log


def joined(earlier, later):
    decay = by_row(jnp.exp(later[1]), later[0].shape[0])
    return earlier[0] * decay + later[0], earlier[1] + later[1]


def write(ref, value, wide_ref):
    ref[: ref.shape[0] - NOTE, :] = value[0].astype(ref.dtype)
    write_log(ref, value[1], wide_ref)


def read_half(both_ref, k):
    half = (both_ref.shape[1] - NOTE) // 2
    core = lax.axis_index("core")
    state = both_ref[k, pl.ds(pl.multiple_of(core * half, half), half), :].astype(F32)
    _, log = read(both_ref[k])
    heads = log.shape[1] // 2
    return state, jnp.where(core == 0, log[:, :heads], log[:, heads:])


def join_core_body(both_ref, out_ref, wide_ref):
    write(out_ref, joined(read_half(both_ref, 0), read_half(both_ref, 1)), wide_ref)


def join_far_body(far_ref, own_ref, log_ref, out_ref):
    rows = far_ref.shape[1] - NOTE
    group, place, core = (lax.axis_index(axis) for axis in EP)
    device = iota(log_ref.shape, 0) // PACK
    logs = log_ref[...].astype(F32)
    heads = rows // HEAD_DIM

    def decay(start, end):
        log = jnp.where((device >= start) & (device < end), logs, 0.0)
        log = jnp.sum(log, axis=0, keepdims=True)
        log = jnp.where(core == 0, log[:, :heads], log[:, heads : 2 * heads])
        return by_row(jnp.exp(log), rows)

    groups, stride = far_ref.shape[0], log_ref.shape[0] // PACK // far_ref.shape[0]
    upto = 2 * place + 2
    state = jnp.zeros((rows, 128), F32)
    for k in range(groups - 1):
        new = state * decay(stride * (k - 1) + upto, stride * k + upto)
        state = jnp.where(k < group, new + far_ref[k, :rows, :].astype(F32), state)
    state = state * decay(stride * (group - 1) + upto, stride * group)
    out_ref[0, :rows, :] = state.astype(BF16)
    out_ref[0, rows:, :] = jnp.zeros((NOTE, 128), BF16)
    out_ref[1] = own_ref[...]


def join_near_body(near_ref, out_ref):
    rows = near_ref.shape[2] - NOTE
    place = lax.axis_index(EP[1])
    state = near_ref[0, 0, :rows, :].astype(F32)
    for k in range(1, near_ref.shape[0]):
        state = state + near_ref[k, 0, :rows, :].astype(F32)
    for k in range(near_ref.shape[0] - 1):
        state = jnp.where(k < place, joined((state, 0.0), read(near_ref[k, 1]))[0], state)
    out_ref[...] = state


def income_of(chips_ref, both_ref):
    state = chips_ref[...]
    inside, _ = joined((state, 0.0), read(both_ref[0]))
    return jnp.where(lax.axis_index("core") == 1, inside, state)


def mixer_body(
    x_ref, b_ref, projection_ref, prior_ref, taps_ref, gate_ref, first_ref, chips_ref, both_ref, step_ref, extra_ref,
    rate_ref, skip_ref, gain_ref, weight_ref, out_ref, normed, income_ref, c_ref, held,
):
    c_ref[...] = conv_silu(projection_ref, prior_ref, taps_ref, 16, held)
    income_ref[...] = income_of(chips_ref, both_ref)
    step_all, log_all = log_decay_of(step_ref, extra_ref, rate_ref)
    wide = (BLOCK, 128)
    causal = iota(wide, 0) >= iota(wide, 1)
    for block in range(x_ref.shape[0] // BLOCK):
        rows, step, decay, last = block_terms(block, step_all, log_all)
        grown = jnp.exp(decay)
        for group in range(x_ref.shape[1] // 128):
            columns = slice(group * 128, (group + 1) * 128)
            a, b = 2 * group, 2 * group + 1
            x = x_ref[rows, columns].astype(F32)
            x_step = (x * pair(step[:, a : a + 1], step[:, b : b + 1], wide, 1)).astype(BF16)
            c = c_ref[rows, columns]
            inner = dot(c, b_ref[rows, columns], 1, 1)
            parts = []
            for head in (a, b):
                along = jnp.broadcast_to(decay[:, head : head + 1], wide)
                distance = along - along.T
                scale = jnp.where(causal, jnp.exp(jnp.where(causal, distance, 0.0)), 0.0)
                parts.append(dot((inner * scale).astype(BF16), x_step))
            y = pair(parts[0], parts[1], wide, 1)
            entering = income_ref[columns, :]
            if block > 0:
                entering = entering * pair(kept[:, a : a + 1], kept[:, b : b + 1], wide, 0)
                entering = entering + first_ref[columns, :]
            off = dot(c, entering.astype(BF16), 1, 1)
            off = off * pair(grown[:, a : a + 1], grown[:, b : b + 1], wide, 1)
            skip = pair(skip_ref[:, a : a + 1], skip_ref[:, b : b + 1], wide, 1)
            mixed = (y + off + skip * x) * silu(gate_ref[rows, columns].astype(F32))
            mean = jnp.sum(mixed * mixed, axis=1, keepdims=True) * (1.0 / 128)
            mixed = mixed * lax.rsqrt(mean + eps) * gain_ref[:, columns]
            normed[rows, columns] = mixed.astype(BF16)
        kept = jnp.exp(last)
    for k in range(0, out_ref.shape[0], 2):
        value = dot(normed[...], weight_ref[:, k * 128 : (k + 2) * 128]).astype(BF16)
        out_ref[k] = value[:, :128]
        out_ref[k + 1] = value[:, 128:]


def all_to_all(value, axis):
    return lax.all_to_all(value, axis, split_axis=0, concat_axis=0, tiled=True)


def per_device(
    mixer_input_channels,
    input_state_projection,
    output_state_projection,
    output_gate_logits,
    step_size_logits,
    extra_log_decay,
    mixer_channel_taps,
    input_state_taps,
    output_state_taps,
    decay_rate_log,
    head_skip_weight,
    grouped_norm_gain,
    mixer_output_weight,
    expert_input_tokens,
    routing,
    router_chosen_scores,
    expert_norm_gain,
    expert_gate_weight,
    expert_up_weight,
    expert_down_weight,
):
    parts = lax.axis_size("tp")
    devices = lax.axis_size(EP)
    length, channels = mixer_input_channels.shape
    tokens, model = expert_input_tokens.shape
    top = routing.shape[1]
    capacity = (tokens * top * 5 + 4 * devices - 1) // (4 * devices)
    message = (devices, PACK, capacity // PACK * LANES)
    noted = (*message[:2], message[2] + LANES)
    folded = pltpu.VMEM((devices * PACK, message[2]), BF16)
    wider = pltpu.VMEM((devices * PACK, noted[2]), BF16)
    slots = devices * capacity
    rate, skip = decay_rate_log[None], head_skip_weight[None]
    step_rows, extra_rows = step_size_logits.T, extra_log_decay.T
    routing_rows = routing.T

    outgoing, edge = kernel_call(
        dispatch_body,
        [shape(noted, BF16), shape((24, channels), BF16)],
        (
            expert_input_tokens, expert_norm_gain[None], routing_rows,
            mixer_input_channels, input_state_projection, output_state_projection,
            step_rows, extra_rows, rate,
        ),
        2 * slots * tokens * 128,
        [wider, pltpu.VMEM((8, LANES), F32)],
        far=(0, 1, 2, 3, 4, 5, 6, 7, 8),
        tails=(3, 4, 5),
        vmem=WHOLE_VMEM,
    )
    prior = lax.ppermute(edge, EP, [(i, i + 1) for i in range(devices - 1)])
    arrived = all_to_all(outgoing, EP)

    note = channels + NOTE
    wide = pltpu.VMEM((NOTE, 128), F32)
    x_conv, b_conv, first, total = kernel_call(
        states_body,
        [shape((length, channels), BF16)] * 2
        + [shape((channels, STATE), F32), shape((note, STATE), BF16)],
        (
            mixer_input_channels, input_state_projection, prior,
            mixer_channel_taps, input_state_taps, step_rows, extra_rows, rate,
        ),
        2 * length * channels * STATE,
        [pltpu.VMEM((length + 8, channels), F32), wide],
        far=(0, 1, 3, 4, 5, 6, 7),
        vmem=WHOLE_VMEM,
    )

    (copies, logs) = kernel_call(
        spread_body,
        [shape((parts, slots, 128), BF16), shape((devices * PACK, LANES), BF16)],
        (arrived,),
        parts * slots * 128,
        [wider, pltpu.VMEM((slots, 128), BF16), pltpu.SemaphoreType.DMA((parts,))],
        out=(pltpu.HBM, pltpu.VMEM),
    )
    gathered = all_to_all(copies, "tp")

    half = channels // 2
    carried = (half + NOTE, STATE)
    both = lax.all_gather(total, "core")
    (chip,) = kernel_call(join_core_body, [shape(carried, BF16)], (both,), 4 * half * STATE, [wide])
    far = lax.all_gather(chip, EP[0])
    (earlier,) = kernel_call(
        join_far_body, [shape((2, *carried), BF16)], (far, chip, logs), 8 * half * STATE
    )
    near = lax.all_gather(earlier, EP[1])
    (chips,) = kernel_call(join_near_body, [shape((half, STATE), F32)], (near,), 8 * half * STATE)
    chips = lax.all_gather(chips, "core", tiled=True)

    (partial_rows,) = kernel_call(
        ffn_body,
        [shape((parts, devices * capacity, 128), BF16)],
        (gathered, expert_gate_weight[0], expert_up_weight[0], expert_down_weight[0]),
        6 * devices * capacity * model * 128,
        [
            pltpu.VMEM((parts, slots, 128), BF16),
            pltpu.SemaphoreType.DMA((parts // 2,)),
        ],
        far=(3,),
        late=(3,),
        out=(pltpu.HBM,),
    )
    expert_parts = all_to_all(partial_rows, "tp")

    (mixer_part,) = kernel_call(
        mixer_body,
        [shape((parts, length, 128), BF16)],
        (
            x_conv, b_conv, output_state_projection, prior, output_state_taps, output_gate_logits, first, chips, both,
            step_rows, extra_rows, rate, skip, grouped_norm_gain[None], mixer_output_weight,
        ),
        2 * length * channels * model,
        [
            pltpu.VMEM((length, channels), BF16), pltpu.VMEM((channels, STATE), F32),
            pltpu.VMEM((length, channels), BF16), pltpu.VMEM((length + 8, channels), F32),
        ],
    )
    mixer_parts = all_to_all(mixer_part, "tp")

    (back,) = kernel_call(
        expert_sum_body, [shape(message, BF16)], (expert_parts,), parts * slots * 128, [folded]
    )
    table = all_to_all(back, EP)

    (mixer_output_first,) = kernel_call(
        sum_body, [shape((length, 128), BF16)], (mixer_parts,), parts * length * 128
    )
    (moe_out,) = kernel_call(
        combine_body,
        [shape((tokens, 128), BF16)],
        (table, routing_rows, router_chosen_scores.T),
        4 * tokens * slots * 128,
        [folded],
    )
    return (mixer_output_first, moe_out)


def solution(mesh):
    split = Mesh(mesh.devices.reshape(4, 4, 2, mesh.shape["tp"]), (*EP, "tp"))
    in_specs = (
        P(EP, "tp"),
        P(EP, "tp"),
        P(EP, "tp"),
        P(EP, "tp"),
        P(EP, "tp"),
        P(EP, "tp"),
        P(None, "tp"),
        P(None, "tp"),
        P(None, "tp"),
        P("tp"),
        P("tp"),
        P("tp"),
        P("tp", None),
        P(EP, None),
        P(EP, None),
        P(EP, None),
        P(),
        P(EP, None, "tp"),
        P(EP, None, "tp"),
        P(EP, "tp", None),
    )
    out_specs = (P(EP, "tp"), P(EP, "tp"))
    return jax.shard_map(
        per_device, mesh=split, in_specs=in_specs, out_specs=out_specs, check_vma=False
    )
```

```python
import jax
import jax.numpy as jnp
from jax import lax
from jax.experimental import pallas as pl
from jax.experimental.pallas import tpu as pltpu
from jax.sharding import Mesh
from jax.sharding import PartitionSpec as P

HEAD_DIM = 64
STATE = 128
BLOCK = 128
EP = ("ep_hi", "ep_lo", "core")
LANES = 128
PACK = 2
NOTE = 16
VMEM = 16 << 20
WHOLE_VMEM = 60 << 20
F32 = jnp.float32
BF16 = jnp.bfloat16

eps = 1e-06


def iota(shape, dim):
    return lax.broadcasted_iota(jnp.int32, shape, dim)


def dot(a, b, ca=1, cb=0, precision=None):
    return lax.dot_general(
        a, b, (((ca,), (cb,)), ((), ())), precision=precision, preferred_element_type=F32
    )


def silu(x):
    return x * (1.0 / (1.0 + jnp.exp(-x)))


def softplus(x):
    return jnp.maximum(x, 0.0) + jnp.log1p(jnp.exp(-jnp.abs(x)))


def fetched(body, ins, outs, own, far, late):
    def whole(*refs):
        given, rest = list(refs[:ins]), refs[ins : ins + outs + own]
        held, sems = refs[ins + outs + own : -1], refs[-1]
        copies = {}
        for k, index in enumerate(far):
            source = given[index]
            if source.shape != held[k].shape:
                source = source.at[pl.ds(source.shape[0] - held[k].shape[0], held[k].shape[0]), :]
            copies[index] = pltpu.make_async_copy(source, held[k], sems.at[k])
            copies[index].start()
            given[index] = held[k]
        for index in far:
            if index not in late:
                copies[index].wait()
        body(*given, *rest, *(copies[index].wait for index in late))

    return whole


def kernel_call(body, outs, args, flops, scratch=(), far=(), late=(), tails=(), vmem=VMEM, out=None):
    out = out or [pltpu.VMEM] * len(outs)
    size = sum(a.size * a.dtype.itemsize for a in args)
    size += sum(o.size * o.dtype.itemsize for o in outs)
    specs = [
        pl.BlockSpec(memory_space=pltpu.HBM if k in far else pltpu.VMEM) for k in range(len(args))
    ]
    scratch = list(scratch)
    if far:
        body = fetched(body, len(args), len(outs), len(scratch), far, late)
        for k in far:
            dims = (8, args[k].shape[1]) if k in tails else args[k].shape
            scratch.append(pltpu.VMEM(dims, args[k].dtype))
        scratch.append(pltpu.SemaphoreType.DMA((len(far),)))
    return pl.pallas_call(
        body,
        out_shape=outs,
        in_specs=specs,
        out_specs=[pl.BlockSpec(memory_space=kind) for kind in out],
        scratch_shapes=scratch,
        cost_estimate=pl.CostEstimate(flops=flops, bytes_accessed=size, transcendentals=0),
        compiler_params=pltpu.CompilerParams(vmem_limit_bytes=vmem),
    )(*args)


def shape(dims, kind):
    return jax.ShapeDtypeStruct(dims, kind)


def upright(ref):
    wide = jnp.concatenate([ref[...].astype(F32)] * (8 // ref.shape[0]), axis=0)
    return wide.T[:, : ref.shape[0]]


def slots_of(routing_ref, experts):
    tokens = routing_ref.shape[1]
    expert = iota((tokens, 128), 1)
    named = upright(routing_ref).astype(jnp.int32)
    first = expert == named[:, 0:1]
    second = expert == named[:, 1:2]
    member = jnp.where(first | second, 1.0, 0.0).astype(BF16)
    earlier = jnp.where(iota((tokens, tokens), 0) > iota((tokens, tokens), 1), 1.0, 0.0)
    place = dot(earlier.astype(BF16), member)
    slots = []
    for index, chosen in enumerate((first, second)):
        rank = jnp.sum(jnp.where(chosen, place, 0.0), axis=1, keepdims=True).astype(jnp.int32)
        number = named[:, index : index + 1] * PACK + rank % PACK
        slots.append(rank // PACK * (PACK * experts) + number)
    return slots


def slots_along(routing_ref, experts):
    tokens = routing_ref.shape[1]
    expert = iota((experts, tokens), 0)
    named = [routing_ref[k : k + 1, :] for k in range(routing_ref.shape[0])]
    chosen = [expert == name for name in named]
    member = jnp.where(chosen[0] | chosen[1], 1.0, 0.0).astype(BF16)
    earlier = jnp.where(iota((tokens, tokens), 0) < iota((tokens, tokens), 1), 1.0, 0.0)
    place = dot(member, earlier.astype(BF16))
    slots = []
    for name, mask in zip(named, chosen):
        rank = jnp.sum(jnp.where(mask, place, 0.0), axis=0, keepdims=True).astype(jnp.int32)
        slots.append(rank // PACK * (PACK * experts) + name * PACK + rank % PACK)
    return slots


def pack_rows(rows, held, out_ref):
    experts = out_ref.shape[0]
    span = PACK * experts
    for k in range(rows.shape[0] // span):
        held[:, k * LANES : (k + 1) * LANES] = rows[k * span : (k + 1) * span, :]
    for e in range(experts):
        out_ref[e] = held[PACK * e : PACK * (e + 1), :]


def unpack_rows(in_ref, held, width):
    for e in range(in_ref.shape[0]):
        held[PACK * e : PACK * (e + 1), :] = in_ref[e]
    parts = [held[:, k : k + LANES] for k in range(0, width, LANES)]
    return jnp.concatenate(parts, axis=0)


def log_decay_of(step_ref, extra_ref, rate_ref):
    step = softplus(upright(step_ref))
    return step, step * -jnp.exp(rate_ref[...]) + upright(extra_ref)


def dispatch_body(
    tok_ref, gain_ref, routing_ref, x_ref, b_ref, c_ref, step_ref, extra_ref, rate_ref,
    out_ref, edge_ref, held, wide_ref, wait,
):
    tokens, model = tok_ref.shape
    experts = out_ref.shape[0]
    width = out_ref.shape[2] - LANES
    for k, ref in enumerate((x_ref, b_ref, c_ref)):
        edge_ref[8 * k : 8 * k + 8, :] = ref[...]
    _, log = log_decay_of(step_ref, extra_ref, rate_ref)
    log = jnp.sum(log, axis=0, keepdims=True)
    high = log.astype(BF16).astype(F32)
    wide_ref[...] = jnp.zeros_like(wide_ref)
    wide_ref[0:1, 0 : log.shape[1]] = high
    wide_ref[1:2, 0 : log.shape[1]] = log - high
    first = iota((experts * PACK, LANES), 0) % PACK == 0
    held[:, width:] = jnp.where(first, wide_ref[0:1, :], wide_ref[1:2, :]).astype(BF16)
    slots = slots_along(routing_ref, experts)
    place = iota((PACK * experts * width // LANES, tokens), 0)
    pick = jnp.where((place == slots[0]) | (place == slots[1]), 1.0, 0.0).astype(BF16)
    wait()
    rows = tok_ref[...].astype(F32)
    scale = lax.rsqrt(jnp.sum(rows * rows, axis=1, keepdims=True) * (1.0 / model) + eps)
    columns = pl.ds(pl.multiple_of(lax.axis_index("tp") * 128, 128), 128)
    own = (tok_ref[:, columns].astype(F32) * scale * gain_ref[:, columns]).astype(BF16)
    pack_rows(dot(pick, own).astype(BF16), held, out_ref)


def spread_body(in_ref, out_ref, log_ref, held, packed, sems):
    width = in_ref.shape[2] - LANES
    packed[...] = unpack_rows(in_ref, held, width)
    log_ref[...] = held[:, width:]
    copies = [
        pltpu.make_async_copy(packed, out_ref.at[peer], sems.at[peer])
        for peer in range(out_ref.shape[0])
    ]
    for copy in copies:
        copy.start()
    for copy in copies:
        copy.wait()


def ffn_body(in_ref, gate_ref, up_ref, down_ref, out_ref, held, sems, wait):
    parts, rows, width = in_ref.shape
    total = jnp.zeros((rows, 2 * width), F32)
    for k in range(0, parts, 2):
        left = jnp.concatenate([in_ref[k], in_ref[k + 1]], axis=1)
        span = pl.ds(k * width, 2 * width)
        right = jnp.concatenate([gate_ref[span, :], up_ref[span, :]], axis=1)
        total = total + dot(left, right)
    hidden = (silu(total[:, :width]) * total[:, width:]).astype(BF16)
    wait()
    copies = []
    for k in range(0, parts, 2):
        value = dot(hidden, down_ref[:, k * width : (k + 2) * width]).astype(BF16)
        held[k] = value[:, :width]
        held[k + 1] = value[:, width:]
        if copies:
            copies[-1].start()
        both = pl.ds(k, 2)
        copies.append(pltpu.make_async_copy(held.at[both], out_ref.at[both], sems.at[k // 2]))
    copies[-1].start()
    for copy in copies:
        copy.wait()


def sum_of(in_ref):
    total = in_ref[0].astype(F32)
    for k in range(1, in_ref.shape[0]):
        total = total + in_ref[k].astype(F32)
    return total.astype(BF16)


def expert_sum_body(in_ref, out_ref, held):
    pack_rows(sum_of(in_ref), held, out_ref)


def sum_body(in_ref, out_ref):
    out_ref[...] = sum_of(in_ref)


def combine_body(table_ref, routing_ref, score_ref, out_ref, held):
    tokens = routing_ref.shape[1]
    scores = upright(score_ref)
    whole = scores[:, 0:1] + scores[:, 1:2]
    table = unpack_rows(table_ref, held, table_ref.shape[2])
    place = iota((tokens, table.shape[0]), 1)
    total = jnp.zeros(out_ref.shape, F32)
    for index, slot in enumerate(slots_of(routing_ref, table_ref.shape[0])):
        pick = jnp.where(place == slot, 1.0, 0.0).astype(BF16)
        total = total + scores[:, index : index + 1] / whole * dot(pick, table)
    out_ref[...] = total.astype(BF16)


def conv_silu(values_ref, prior_ref, taps_ref, start, held):
    length = values_ref.shape[0]
    reach = taps_ref.shape[0] - 1
    held[0:8, :] = prior_ref[start : start + 8, :].astype(F32)
    held[8 : 8 + length, :] = values_ref[...].astype(F32)
    total = jnp.zeros(values_ref.shape, F32)
    for k in range(reach + 1):
        total = total + held[8 - reach + k : 8 - reach + k + length, :] * taps_ref[
            k : k + 1, :
        ].astype(F32)
    return silu(total).astype(BF16)


def running_sum(values):
    length = values.shape[0]
    reach = 1
    row = iota(values.shape, 0)
    while reach < length:
        moved = pltpu.roll(values, reach, 0)
        values = values + jnp.where(row >= reach, moved, 0.0)
        reach *= 2
    return values


def pair(left, right, dims, dim):
    return jnp.where(iota(dims, dim) < HEAD_DIM, left, right)


def block_terms(block, step_all, log_all):
    rows = slice(block * BLOCK, (block + 1) * BLOCK)
    step = step_all[rows]
    decay = running_sum(log_all[rows])
    return rows, step, decay, decay[BLOCK - 1 : BLOCK, :]


def states_body(
    x_ref, b_ref, prior_ref, xt_ref, bt_ref, step_ref, extra_ref, rate_ref,
    xo_ref, bo_ref, first_ref, total_ref, held, wide_ref,
):
    xo_ref[...] = conv_silu(x_ref, prior_ref, xt_ref, 0, held)
    bo_ref[...] = conv_silu(b_ref, prior_ref, bt_ref, 8, held)
    step_all, log_all = log_decay_of(step_ref, extra_ref, rate_ref)
    wide = (BLOCK, 128)
    for group in range(x_ref.shape[1] // 128):
        columns = slice(group * 128, (group + 1) * 128)
        a, b = 2 * group, 2 * group + 1
        state = None
        for block in range(x_ref.shape[0] // BLOCK):
            rows, step, decay, last = block_terms(block, step_all, log_all)
            x = xo_ref[rows, columns].astype(F32)
            x_step = (x * pair(step[:, a : a + 1], step[:, b : b + 1], wide, 1)).astype(BF16)
            left = jnp.exp(last - decay)
            weighted = x_step.astype(F32) * pair(left[:, a : a + 1], left[:, b : b + 1], wide, 1)
            new = dot(weighted.astype(BF16), bo_ref[rows, columns], 0, 0)
            if state is None:
                first_ref[columns, :] = new
                state = new
            else:
                kept = jnp.exp(last)
                state = state * pair(kept[:, a : a + 1], kept[:, b : b + 1], wide, 0) + new
        total_ref[columns, :] = state.astype(BF16)
    write_log(total_ref, jnp.sum(log_all, axis=0, keepdims=True), wide_ref)


def write_log(ref, log, wide_ref):
    rows = ref.shape[0] - NOTE
    wide_ref[...] = jnp.zeros_like(wide_ref)
    for part in range(3):
        piece = log.astype(ref.dtype).astype(F32)
        wide_ref[part : part + 1, 0 : log.shape[1]] = piece
        log = log - piece
    ref[rows:, :] = wide_ref[...].astype(ref.dtype)


def by_row(values, rows):
    head = iota((rows, 128), 0) // HEAD_DIM
    total = jnp.broadcast_to(values[:, 0:1], (rows, 128))
    for k in range(1, values.shape[1]):
        total = jnp.where(head == k, values[:, k : k + 1], total)
    return total


def read(part):
    rows = part.shape[0] - NOTE
    note = part[rows:, :].astype(F32)
    log = (note[0:1] + note[1:2] + note[2:3])[:, : rows // HEAD_DIM]
    return part[:rows, :].astype(F32), log


def joined(earlier, later):
    decay = by_row(jnp.exp(later[1]), later[0].shape[0])
    return earlier[0] * decay + later[0], earlier[1] + later[1]


def write(ref, value, wide_ref):
    ref[: ref.shape[0] - NOTE, :] = value[0].astype(ref.dtype)
    write_log(ref, value[1], wide_ref)


def read_half(both_ref, k):
    half = (both_ref.shape[1] - NOTE) // 2
    core = lax.axis_index("core")
    state = both_ref[k, pl.ds(pl.multiple_of(core * half, half), half), :].astype(F32)
    _, log = read(both_ref[k])
    heads = log.shape[1] // 2
    return state, jnp.where(core == 0, log[:, :heads], log[:, heads:])


def join_core_body(both_ref, out_ref, state_ref, wide_ref):
    chip = joined(read_half(both_ref, 0), read_half(both_ref, 1))
    write(out_ref, chip, wide_ref)
    state_ref[...] = chip[0].astype(BF16)


def join_far_body(far_ref, own_ref, log_ref, out_ref):
    rows = far_ref.shape[1]
    group, place, core = (lax.axis_index(axis) for axis in EP)
    device = iota(log_ref.shape, 0) // PACK
    logs = log_ref[...].astype(F32)
    heads = rows // HEAD_DIM

    def decay(start, end):
        log = jnp.where((device >= start) & (device < end), logs, 0.0)
        log = jnp.sum(log, axis=0, keepdims=True)
        log = jnp.where(core == 0, log[:, :heads], log[:, heads : 2 * heads])
        return by_row(jnp.exp(log), rows)

    groups, stride = far_ref.shape[0], log_ref.shape[0] // PACK // far_ref.shape[0]
    upto = 2 * place + 2
    state = jnp.zeros((rows, 128), F32)
    for k in range(groups - 1):
        new = state * decay(stride * (k - 1) + upto, stride * k + upto)
        state = jnp.where(k < group, new + far_ref[k, :rows, :].astype(F32), state)
    state = state * decay(stride * (group - 1) + upto, stride * group)
    out_ref[0, :rows, :] = state.astype(BF16)
    out_ref[0, rows:, :] = jnp.zeros((NOTE, 128), BF16)
    out_ref[1] = own_ref[...]


def join_near_body(near_ref, out_ref):
    rows = near_ref.shape[2] - NOTE
    place = lax.axis_index(EP[1])
    state = near_ref[0, 0, :rows, :].astype(F32)
    for k in range(1, near_ref.shape[0]):
        state = state + near_ref[k, 0, :rows, :].astype(F32)
    for k in range(near_ref.shape[0] - 1):
        state = jnp.where(k < place, joined((state, 0.0), read(near_ref[k, 1]))[0], state)
    out_ref[...] = state


def income_of(chips_ref, both_ref):
    state = chips_ref[...]
    inside, _ = joined((state, 0.0), read(both_ref[0]))
    return jnp.where(lax.axis_index("core") == 1, inside, state)


def mixer_body(
    x_ref, b_ref, projection_ref, prior_ref, taps_ref, gate_ref, first_ref, chips_ref, both_ref, step_ref, extra_ref,
    rate_ref, skip_ref, gain_ref, weight_ref, out_ref, normed, income_ref, c_ref, held,
):
    c_ref[...] = conv_silu(projection_ref, prior_ref, taps_ref, 16, held)
    income_ref[...] = income_of(chips_ref, both_ref)
    step_all, log_all = log_decay_of(step_ref, extra_ref, rate_ref)
    wide = (BLOCK, 128)
    causal = iota(wide, 0) >= iota(wide, 1)
    for block in range(x_ref.shape[0] // BLOCK):
        rows, step, decay, last = block_terms(block, step_all, log_all)
        grown = jnp.exp(decay)
        for group in range(x_ref.shape[1] // 128):
            columns = slice(group * 128, (group + 1) * 128)
            a, b = 2 * group, 2 * group + 1
            x = x_ref[rows, columns].astype(F32)
            x_step = (x * pair(step[:, a : a + 1], step[:, b : b + 1], wide, 1)).astype(BF16)
            c = c_ref[rows, columns]
            inner = dot(c, b_ref[rows, columns], 1, 1)
            parts = []
            for head in (a, b):
                along = jnp.broadcast_to(decay[:, head : head + 1], wide)
                distance = along - along.T
                scale = jnp.where(causal, jnp.exp(jnp.where(causal, distance, 0.0)), 0.0)
                parts.append(dot((inner * scale).astype(BF16), x_step))
            y = pair(parts[0], parts[1], wide, 1)
            entering = income_ref[columns, :]
            if block > 0:
                entering = entering * pair(kept[:, a : a + 1], kept[:, b : b + 1], wide, 0)
                entering = entering + first_ref[columns, :]
            off = dot(c, entering.astype(BF16), 1, 1)
            off = off * pair(grown[:, a : a + 1], grown[:, b : b + 1], wide, 1)
            skip = pair(skip_ref[:, a : a + 1], skip_ref[:, b : b + 1], wide, 1)
            mixed = (y + off + skip * x) * silu(gate_ref[rows, columns].astype(F32))
            mean = jnp.sum(mixed * mixed, axis=1, keepdims=True) * (1.0 / 128)
            mixed = mixed * lax.rsqrt(mean + eps) * gain_ref[:, columns]
            normed[rows, columns] = mixed.astype(BF16)
        kept = jnp.exp(last)
    for k in range(0, out_ref.shape[0], 2):
        value = dot(normed[...], weight_ref[:, k * 128 : (k + 2) * 128]).astype(BF16)
        out_ref[k] = value[:, :128]
        out_ref[k + 1] = value[:, 128:]


def all_to_all(value, axis):
    return lax.all_to_all(value, axis, split_axis=0, concat_axis=0, tiled=True)


def per_device(
    mixer_input_channels,
    input_state_projection,
    output_state_projection,
    output_gate_logits,
    step_size_logits,
    extra_log_decay,
    mixer_channel_taps,
    input_state_taps,
    output_state_taps,
    decay_rate_log,
    head_skip_weight,
    grouped_norm_gain,
    mixer_output_weight,
    expert_input_tokens,
    routing,
    router_chosen_scores,
    expert_norm_gain,
    expert_gate_weight,
    expert_up_weight,
    expert_down_weight,
):
    parts = lax.axis_size("tp")
    devices = lax.axis_size(EP)
    length, channels = mixer_input_channels.shape
    tokens, model = expert_input_tokens.shape
    top = routing.shape[1]
    capacity = (tokens * top * 5 + 4 * devices - 1) // (4 * devices)
    message = (devices, PACK, capacity // PACK * LANES)
    noted = (*message[:2], message[2] + LANES)
    folded = pltpu.VMEM((devices * PACK, message[2]), BF16)
    wider = pltpu.VMEM((devices * PACK, noted[2]), BF16)
    slots = devices * capacity
    rate, skip = decay_rate_log[None], head_skip_weight[None]
    step_rows, extra_rows = step_size_logits.T, extra_log_decay.T
    routing_rows = routing.T

    outgoing, edge = kernel_call(
        dispatch_body,
        [shape(noted, BF16), shape((24, channels), BF16)],
        (
            expert_input_tokens, expert_norm_gain[None], routing_rows,
            mixer_input_channels, input_state_projection, output_state_projection,
            step_rows, extra_rows, rate,
        ),
        2 * slots * tokens * 128,
        [wider, pltpu.VMEM((8, LANES), F32)],
        far=(0, 1, 2, 3, 4, 5, 6, 7, 8),
        late=(0,),
        tails=(3, 4, 5),
        vmem=WHOLE_VMEM,
    )
    prior = lax.ppermute(edge, EP, [(i, i + 1) for i in range(devices - 1)])
    arrived = all_to_all(outgoing, EP)

    note = channels + NOTE
    wide = pltpu.VMEM((NOTE, 128), F32)
    x_conv, b_conv, first, total = kernel_call(
        states_body,
        [shape((length, channels), BF16)] * 2
        + [shape((channels, STATE), F32), shape((note, STATE), BF16)],
        (
            mixer_input_channels, input_state_projection, prior,
            mixer_channel_taps, input_state_taps, step_rows, extra_rows, rate,
        ),
        2 * length * channels * STATE,
        [pltpu.VMEM((length + 8, channels), F32), wide],
        far=(0, 1, 3, 4, 5, 6, 7),
        vmem=WHOLE_VMEM,
    )

    (copies, logs) = kernel_call(
        spread_body,
        [shape((parts, slots, 128), BF16), shape((devices * PACK, LANES), BF16)],
        (arrived,),
        parts * slots * 128,
        [wider, pltpu.VMEM((slots, 128), BF16), pltpu.SemaphoreType.DMA((parts,))],
        out=(pltpu.HBM, pltpu.VMEM),
    )
    gathered = all_to_all(copies, "tp")

    half = channels // 2
    carried = (half + NOTE, STATE)
    both = lax.all_gather(total, "core")
    outs = [shape(carried, BF16), shape((half, STATE), BF16)]
    chip, state = kernel_call(join_core_body, outs, (both,), 4 * half * STATE, [wide])
    far = lax.all_gather(state, EP[0])
    (earlier,) = kernel_call(
        join_far_body, [shape((2, *carried), BF16)], (far, chip, logs), 8 * half * STATE
    )
    near = lax.all_gather(earlier, EP[1])
    (chips,) = kernel_call(join_near_body, [shape((half, STATE), F32)], (near,), 8 * half * STATE)
    chips = lax.all_gather(chips, "core", tiled=True)

    (partial_rows,) = kernel_call(
        ffn_body,
        [shape((parts, devices * capacity, 128), BF16)],
        (gathered, expert_gate_weight[0], expert_up_weight[0], expert_down_weight[0]),
        6 * devices * capacity * model * 128,
        [
            pltpu.VMEM((parts, slots, 128), BF16),
            pltpu.SemaphoreType.DMA((parts // 2,)),
        ],
        far=(3,),
        late=(3,),
        out=(pltpu.HBM,),
    )
    expert_parts = all_to_all(partial_rows, "tp")

    (mixer_part,) = kernel_call(
        mixer_body,
        [shape((parts, length, 128), BF16)],
        (
            x_conv, b_conv, output_state_projection, prior, output_state_taps, output_gate_logits, first, chips, both,
            step_rows, extra_rows, rate, skip, grouped_norm_gain[None], mixer_output_weight,
        ),
        2 * length * channels * model,
        [
            pltpu.VMEM((length, channels), BF16), pltpu.VMEM((channels, STATE), F32),
            pltpu.VMEM((length, channels), BF16), pltpu.VMEM((length + 8, channels), F32),
        ],
    )
    mixer_parts = all_to_all(mixer_part, "tp")

    (back,) = kernel_call(
        expert_sum_body, [shape(message, BF16)], (expert_parts,), parts * slots * 128, [folded]
    )
    table = all_to_all(back, EP)

    (mixer_output_first,) = kernel_call(
        sum_body, [shape((length, 128), BF16)], (mixer_parts,), parts * length * 128
    )
    (moe_out,) = kernel_call(
        combine_body,
        [shape((tokens, 128), BF16)],
        (table, routing_rows, router_chosen_scores.T),
        4 * tokens * slots * 128,
        [folded],
    )
    return (mixer_output_first, moe_out)


def solution(mesh):
    split = Mesh(mesh.devices.reshape(4, 4, 2, mesh.shape["tp"]), (*EP, "tp"))
    in_specs = (
        P(EP, "tp"),
        P(EP, "tp"),
        P(EP, "tp"),
        P(EP, "tp"),
        P(EP, "tp"),
        P(EP, "tp"),
        P(None, "tp"),
        P(None, "tp"),
        P(None, "tp"),
        P("tp"),
        P("tp"),
        P("tp"),
        P("tp", None),
        P(EP, None),
        P(EP, None),
        P(EP, None),
        P(),
        P(EP, None, "tp"),
        P(EP, None, "tp"),
        P(EP, "tp", None),
    )
    out_specs = (P(EP, "tp"), P(EP, "tp"))
    return jax.shard_map(
        per_device, mesh=split, in_specs=in_specs, out_specs=out_specs, check_vma=False
    )
```
